32 devices in a mesh: ep: 16 (over z, y, x), tp: 2 (over core).
Axes of the slice: x: 2, y: 2, z: 4, core: 2. Of those that a mesh axis runs over, the one named last changes fastest.
Arguments:
- tokens: bfloat16 [384, 2048], P('ep'), may hold values from -6 to 6
- norm_gain: bfloat16 [2048], replicated, may hold values from 0.099609375 to 1.8984375
- query_w: bfloat16 [2048, 1024], P(None, 'tp'), may hold values from -0.125 to 0.125
- key_w: bfloat16 [2048, 128], replicated, may hold values from -0.125 to 0.125
- value_w: bfloat16 [2048, 128], replicated, may hold values from -0.125 to 0.125
- forget_w: bfloat16 [2048, 16], replicated, may hold values from -0.125 to 0.125
- forget_bias: float32 [16], replicated, may hold values from 0 to 4
- query_gain: bfloat16 [64], replicated, may hold values from 0.099609375 to 1.8984375
- key_gain: bfloat16 [64], replicated, may hold values from 0.099609375 to 1.8984375
- cache_key: bfloat16 [384, 2, 64, 1024], P('ep', 'tp'), may hold values from -6 to 6
- cache_value: bfloat16 [384, 2, 64, 1024], P('ep', 'tp'), may hold values from -6 to 6
- cache_gate: float32 [384, 16, 1024], P('ep', 'tp'), may hold values from -105 to 0, as said below
- cache_len: int32 [384], P('ep'), may hold values from 256 to 1024
- out_w: bfloat16 [1024, 2048], P('tp'), may hold values from -0.1875 to 0.1875
- post_gain: bfloat16 [2048], replicated, may hold values from 0.099609375 to 1.8984375
- branch_gate: bfloat16 [2048], replicated, may hold values from -0.125 to 0.125
- dense_gate_w: bfloat16 [2048, 16384], P(None, ('ep', 'tp')), may hold values from -0.125 to 0.125
- dense_up_w: bfloat16 [2048, 16384], P(None, ('ep', 'tp')), may hold values from -1.3258252 to 1.3258252
- dense_down_w: bfloat16 [16384, 2048], P(('ep', 'tp')), may hold values from -0.046875 to 0.046875
- expert_choice: int32 [384, 2], P('ep'), may hold values from 0 to 15, as said below
- route_weight: float32 [384, 2], P('ep'), may hold values from 0.1 to 1
- expert_gate_w: bfloat16 [16, 2048, 1024], P('ep', None, 'tp'), may hold values from -0.125 to 0.125
- expert_up_w: bfloat16 [16, 2048, 1024], P('ep', None, 'tp'), may hold values from -0.125 to 0.125
- expert_down_w: bfloat16 [16, 1024, 2048], P('ep', 'tp'), may hold values from -0.1875 to 0.1875
Outputs:
- mixed_out: bfloat16 [384, 2048], P('ep', 'tp')
- fresh_key: bfloat16 [384, 2, 64], P('ep', 'tp')
- fresh_value: bfloat16 [384, 2, 64], P('ep', 'tp')
- fresh_gate: float32 [384, 16], P('ep', 'tp')
The draws below stay inside these ranges and needn't reach their ends.
Inputs may be any that keep to these rules, and one draw needn't show every extreme that they name: `cache_gate`: Non-increasing along positions. `expert_choice`: experts 4 * g to 4 * g + 3 form group g. A token names 2 different experts of one group. Among the 24 tokens of one index of ep, those at even offsets all choose one group and the others choose other groups; no expert is named more than 6 times by them, and some expert exactly 6 times.
All inputs are finite; a program needn't handle non-finite values.
Results may differ from the reference program's by a relative error of at most 0.014.
Values may be sent and summed in bfloat16 or wider, within the bound.
No kernel may reach another device: no remote copies, remote signals or barrier semaphores. Data moves between devices by JAX's collectives and lax.ppermute only.
A program may use at most 128 MiB of HBM per device.

```python
import math
import jax
import jax.numpy as jnp
from jax import lax

D = 2048
HEADS = 16
KV = 2
HD = 64
FFE = 1024
FF2 = 16384
GROUPS = 4
TOPK = 2
SEQ_DEV = 24
STORED_SLOTS = 1024
BATCH_ENTRIES = 384
EXPERTS = 16
EPG = 4
CAP = 6
N_EP = 16
N_TP = 2


def draw_cache_gate(key, part):
    derived_prng_seeds = jax.random.split(jax.random.fold_in(key, 11), 7)
    fast_share = 0.5
    is_fast = jax.random.uniform(derived_prng_seeds[0], (HEADS,)) < fast_share
    slow_rate = jax.random.uniform(derived_prng_seeds[1], (HEADS,), minval=0.3, maxval=0.8) / STORED_SLOTS
    fast_rate = 1.0 / jax.random.uniform(derived_prng_seeds[2], (HEADS,), minval=30.0, maxval=100.0)
    per_attender_fading = jnp.where(is_fast, fast_rate, slow_rate)
    batch_multiplier = jnp.exp(jax.random.uniform(derived_prng_seeds[3], (BATCH_ENTRIES, 1, 1), minval=math.log(0.6), maxval=math.log(1.6)))
    outer_level_logits = jax.random.uniform(derived_prng_seeds[4], (BATCH_ENTRIES, HEADS, STORED_SLOTS), minval=0.5, maxval=1.5)
    contiguous_first_slot = jax.random.randint(derived_prng_seeds[5], (BATCH_ENTRIES, 3), 0, STORED_SLOTS)
    contiguous_span = jax.random.uniform(derived_prng_seeds[6], (BATCH_ENTRIES, 3), minval=0.22, maxval=0.69)
    current_slot_offset = jnp.arange(STORED_SLOTS)[None, None, :]
    contiguous_tiles = jnp.sum(jnp.where(current_slot_offset == contiguous_first_slot[:, :, None], contiguous_span[:, :, None], 0.0), axis=1)
    increment_fading_exponent = -(per_attender_fading[None, :, None] * batch_multiplier * outer_level_logits) - contiguous_tiles[:, None, :]
    return jnp.cumsum(increment_fading_exponent, axis=2).astype(jnp.float32)


def draw_dense_up_w(key, part):
    base_key = jax.random.fold_in(key, 21)
    column = jnp.arange(FF2, dtype=jnp.float32) / FF2
    entries = jnp.clip(jax.random.normal(base_key, (D, FF2)), -6.0, 6.0)
    column_scale = jnp.exp(math.log(10.0) * column)
    return (entries * column_scale[None, :] * D ** (-0.5)).astype(jnp.bfloat16)


def draw_expert_choice(key, part):
    derived_prng_seeds = jax.random.split(jax.random.fold_in(key, 31), 3)
    blocks = BATCH_ENTRIES // SEQ_DEV
    even_group = jax.random.randint(derived_prng_seeds[0], (blocks, 1), 0, GROUPS)
    other_group = (even_group + 1 + jax.random.randint(derived_prng_seeds[1], (blocks, SEQ_DEV), 0, GROUPS - 1)) % GROUPS
    offset = jnp.arange(SEQ_DEV)[None, :]
    group_id = jnp.where(offset % 2 == 0, even_group, other_group)
    member_of = (group_id[:, :, None] == jnp.arange(GROUPS)[None, None, :]).astype(jnp.int32)
    rank_in = jnp.sum((jnp.cumsum(member_of, axis=1) - member_of) * member_of, axis=2)
    shift_by = jax.random.randint(derived_prng_seeds[2], (blocks, GROUPS), 0, EPG)
    start_at = jnp.sum(member_of * shift_by[:, None, :], axis=2)
    first_member = (start_at + rank_in) % EPG
    second = (first_member + 1) % EPG
    chosen = jnp.stack([group_id * EPG + first_member, group_id * EPG + second], axis=-1)
    return chosen.reshape(BATCH_ENTRIES, TOPK).astype(jnp.int32)


def place_ends(values, stream_key, least, high):
    dims = values.shape
    spot = [jax.random.randint(jax.random.fold_in(stream_key, axis), (), 0, dims[axis]) for axis in range(len(dims))]
    values = values.at[tuple(spot)].set(least)
    longest = dims.index(max(dims))
    spot[longest] = (spot[longest] + 1) % dims[longest]
    return values.at[tuple(spot)].set(high)


def levels(own_key, dims, cuts, smallest, top_value):
    level, own = 1.0, jax.random.fold_in(own_key, 6)
    for axis_at, blocks in cuts:
        steps = jnp.exp(jax.random.uniform(jax.random.fold_in(own, axis_at), (blocks,), jnp.float32, smallest / len(cuts), top_value / len(cuts)))
        level = level * jnp.repeat(steps, dims[axis_at] // blocks).reshape([-1 if axis == axis_at else 1 for axis in range(len(dims))])
    return level


def bell_draw(key, dims, scale, reach, pieces=(), held_as=jnp.bfloat16):
    values = scale * jax.random.normal(key, dims, jnp.float32)
    if pieces:
        values = values * levels(key, dims, pieces, -0.22, 0.18)
    return jnp.clip(values, -reach, reach).astype(held_as)


def setup_inputs(seed: int = 0) -> dict:
    streams_of = jax.random.split(jax.random.key(seed), 25)
    return {
        "tokens": bell_draw(streams_of[0], (BATCH_ENTRIES, D), 1.0, 6.0, ((0, 16),)),
        "norm_gain": jnp.clip(1.0 + 0.18 * jax.random.normal(streams_of[1], (D,), jnp.float32), 0.099609375, 1.8984375).astype(jnp.bfloat16),
        "query_w": bell_draw(streams_of[2], (D, HEADS * HD), D ** -0.5, 0.125, ((1, 2),)),
        "key_w": bell_draw(streams_of[3], (D, KV * HD), D ** -0.5, 0.125),
        "value_w": bell_draw(streams_of[4], (D, KV * HD), D ** -0.5, 0.125),
        "forget_w": bell_draw(streams_of[5], (D, HEADS), D ** -0.5, 0.125),
        "forget_bias": jnp.clip(jax.random.uniform(streams_of[6], (HEADS,), jnp.float32, 0.0, 4.0), 0.0, 4.0),
        "query_gain": jnp.clip(1.0 + 0.18 * jax.random.normal(streams_of[7], (HD,), jnp.float32), 0.099609375, 1.8984375).astype(jnp.bfloat16),
        "key_gain": jnp.clip(1.0 + 0.18 * jax.random.normal(streams_of[8], (HD,), jnp.float32), 0.099609375, 1.8984375).astype(jnp.bfloat16),
        "cache_key": bell_draw(streams_of[9], (BATCH_ENTRIES, KV, HD, STORED_SLOTS), 1.0, 6.0, ((0, 16), (1, 2))),
        "cache_value": bell_draw(streams_of[10], (BATCH_ENTRIES, KV, HD, STORED_SLOTS), 1.0, 6.0, ((0, 16), (1, 2))),
        "cache_gate": draw_cache_gate(jax.random.fold_in(streams_of[24], 71), 0),
        "cache_len": place_ends(jax.random.randint(streams_of[12], (BATCH_ENTRIES,), STORED_SLOTS // 4, STORED_SLOTS + 1), jax.random.fold_in(streams_of[12], 1), STORED_SLOTS // 4, STORED_SLOTS).astype(jnp.int32),
        "out_w": bell_draw(streams_of[13], (HEADS * HD, D), (HEADS * HD) ** -0.5, 0.1875, ((0, 2),)),
        "post_gain": jnp.clip(1.0 + 0.18 * jax.random.normal(streams_of[14], (D,), jnp.float32), 0.099609375, 1.8984375).astype(jnp.bfloat16),
        "branch_gate": bell_draw(streams_of[15], (D,), D ** -0.5, 0.125),
        "dense_gate_w": bell_draw(streams_of[16], (D, FF2), D ** -0.5, 0.125, ((1, 32),)),
        "dense_up_w": draw_dense_up_w(jax.random.fold_in(streams_of[24], 71), 0),
        "dense_down_w": bell_draw(streams_of[18], (FF2, D), FF2 ** -0.5, 0.046875, ((0, 32),)),
        "expert_choice": draw_expert_choice(jax.random.fold_in(streams_of[24], 71), 0),
        "route_weight": jnp.clip(0.1 + 0.9 * jax.random.uniform(streams_of[20], (BATCH_ENTRIES, TOPK), jnp.float32) ** levels(streams_of[20], (BATCH_ENTRIES, TOPK), ((0, 16),), -0.2, 0.2), 0.1, 1.0),
        "expert_gate_w": bell_draw(streams_of[21], (EXPERTS, D, FFE), D ** -0.5, 0.125, ((0, 16), (2, 2))),
        "expert_up_w": bell_draw(streams_of[22], (EXPERTS, D, FFE), D ** -0.5, 0.125, ((0, 16), (2, 2))),
        "expert_down_w": bell_draw(streams_of[23], (EXPERTS, FFE, D), FFE ** -0.5, 0.1875, ((0, 16), (1, 2))),
    }


norm_eps = 1e-06

def rms_scale(values, gain_vec):
    mean_square = lax.optimization_barrier(jnp.mean(values * values, axis=-1, keepdims=True))
    return values * lax.rsqrt(mean_square + norm_eps) * gain_vec

def rounded(values):
    return lax.optimization_barrier(values.astype(jnp.bfloat16)).astype(jnp.float32)

def attend(block_in):
    queries, new_keys, new_values, log_forget, keys_cached, values_cached, gates_cached, lengths = block_in
    row_count = queries.shape[0]
    repeat = HEADS // KV
    score_scale = HD ** (-0.5)
    grouped = queries.reshape(row_count, KV, repeat, HD).astype(jnp.float32)
    scores = jnp.einsum('sgrd,sgdl->sgrl', grouped, keys_cached.astype(jnp.float32)) * score_scale
    own_score = jnp.einsum('sgrd,sgd->sgr', grouped, new_keys.astype(jnp.float32)) * score_scale
    current_slot_offset = lax.broadcasted_iota(jnp.int32, (row_count, STORED_SLOTS), 1)
    at_last = (current_slot_offset == lengths[:, None] - 1)[:, None, :]
    previous = lax.optimization_barrier(jnp.sum(jnp.where(at_last, gates_cached, jnp.zeros_like(gates_cached)), axis=2))
    current = previous + log_forget
    decay_bias = (current[:, :, None] - gates_cached).reshape(row_count, KV, repeat, STORED_SLOTS)
    is_valid = (current_slot_offset < lengths[:, None])[:, None, None, :]
    logits = jnp.where(is_valid, scores + decay_bias, -jnp.inf)
    top_logit = jnp.maximum(lax.optimization_barrier(jnp.max(logits, axis=3)), own_score)
    weights = jnp.exp(logits - top_logit[..., None])
    own_weight = jnp.exp(own_score - top_logit)
    total_weight = lax.optimization_barrier(jnp.sum(weights, axis=3)) + own_weight
    cache_probs = (weights / total_weight[..., None]).astype(jnp.bfloat16)
    own_prob = (own_weight / total_weight).astype(jnp.bfloat16)
    mixed_heads = jnp.einsum('sgrl,sgdl->sgrd', cache_probs.astype(jnp.float32), values_cached.astype(jnp.float32))
    mixed_heads = mixed_heads + own_prob.astype(jnp.float32)[..., None] * new_values.astype(jnp.float32)[:, :, None, :]
    return (mixed_heads.reshape(row_count, HEADS * HD).astype(jnp.bfloat16), current)

def reference(tokens, norm_gain, query_w, key_w, value_w, forget_w, forget_bias, query_gain, key_gain, cache_key, cache_value, cache_gate, cache_len, out_w, post_gain, branch_gate, dense_gate_w, dense_up_w, dense_down_w, expert_choice, route_weight, expert_gate_w, expert_up_w, expert_down_w):
    token_count = tokens.shape[0]
    resid_in = tokens.astype(jnp.float32)
    normed = rms_scale(resid_in, norm_gain.astype(jnp.float32)).astype(jnp.bfloat16)
    queries = jnp.dot(normed, query_w, preferred_element_type=jnp.float32).reshape(token_count, HEADS, HD)
    queries = rms_scale(queries, query_gain.astype(jnp.float32)).astype(jnp.bfloat16)
    fresh_key = jnp.dot(normed, key_w, preferred_element_type=jnp.float32).reshape(token_count, KV, HD)
    fresh_key = rms_scale(fresh_key, key_gain.astype(jnp.float32)).astype(jnp.bfloat16)
    fresh_value = jnp.dot(normed, value_w, preferred_element_type=jnp.float32).astype(jnp.bfloat16).reshape(token_count, KV, HD)
    log_forget = jax.nn.log_sigmoid(jnp.dot(normed, forget_w, preferred_element_type=jnp.float32) + forget_bias)

    def blocks(array_in):
        return array_in.reshape((N_EP, SEQ_DEV) + array_in.shape[1:])
    heads_out, fresh_gate = lax.map(attend, tuple((blocks(array_in) for array_in in (queries, fresh_key, fresh_value, log_forget, cache_key, cache_value, cache_gate, cache_len))))
    heads_out = heads_out.reshape(token_count, HEADS * HD)
    fresh_gate = fresh_gate.reshape(token_count, HEADS)
    head_groups = heads_out.reshape(token_count, N_TP, -1)
    out_parts = out_w.reshape(N_TP, -1, D)
    attn_sum = jnp.zeros((token_count, D), jnp.float32)
    for group_index in range(N_TP):
        attn_sum = attn_sum + rounded(jnp.dot(head_groups[:, group_index], out_parts[group_index], preferred_element_type=jnp.float32))
    resid_out = rounded(resid_in + attn_sum)
    post_norm = rms_scale(resid_out, post_gain.astype(jnp.float32)).astype(jnp.bfloat16)
    branch = jax.nn.sigmoid(jnp.dot(post_norm, branch_gate, preferred_element_type=jnp.float32))
    hidden = jax.nn.silu(jnp.dot(post_norm, dense_gate_w, preferred_element_type=jnp.float32)) * jnp.dot(post_norm, dense_up_w, preferred_element_type=jnp.float32)
    inverse = lax.rsqrt(lax.optimization_barrier(jnp.mean(hidden * hidden, axis=1)) + norm_eps)
    dense_out = rounded(jnp.dot(hidden.astype(jnp.bfloat16), dense_down_w, preferred_element_type=jnp.float32) * inverse[:, None])
    route_total = token_count * TOPK
    route_ids = expert_choice.reshape(-1).astype(jnp.int32)
    limit = N_EP * CAP

    def one_expert(routed_acc, slices):
        gate_mat, up_mat, down_mat, expert_index = slices
        picked = jnp.nonzero(route_ids == expert_index, size=limit, fill_value=route_total)[0].astype(jnp.int32)
        slot_rows = post_norm[jnp.minimum(picked, route_total - 1) // TOPK]
        gate_val = jnp.dot(slot_rows, gate_mat, preferred_element_type=jnp.float32)
        up_val = jnp.dot(slot_rows, up_mat, preferred_element_type=jnp.float32)
        activated = (jax.nn.silu(gate_val) * up_val).astype(jnp.bfloat16)
        act_parts = activated.reshape(limit, N_TP, -1)
        down_parts = down_mat.reshape(N_TP, -1, D)
        expert_out = jnp.zeros((limit, D), jnp.float32)
        for group_index in range(N_TP):
            expert_out = expert_out + rounded(jnp.dot(act_parts[:, group_index], down_parts[group_index], preferred_element_type=jnp.float32))
        routed_acc = routed_acc.at[picked].set(rounded(expert_out), mode='drop')
        return (routed_acc, None)
    routed, _ = lax.scan(one_expert, jnp.zeros((route_total, D), jnp.float32), (expert_gate_w, expert_up_w, expert_down_w, jnp.arange(N_EP, dtype=jnp.int32)))
    expert_sum = lax.optimization_barrier(jnp.sum(route_weight[:, :, None] * routed.reshape(token_count, TOPK, D), axis=1))
    mixed_out = (resid_out + expert_sum + branch[:, None] * dense_out).astype(jnp.bfloat16)
    return (mixed_out, fresh_key, fresh_value, fresh_gate)
```

```python
import jax
import jax.numpy as jnp
from jax import lax
from jax.sharding import PartitionSpec as P

GROUPS = 4
LANES = 128

norm_eps = 1e-06


def rms_scale(values, gain_vec):
    mean_square = jnp.mean(values * values, axis=-1, keepdims=True)
    return values * lax.rsqrt(mean_square + norm_eps) * gain_vec


def split_two(values):
    high = values.astype(jnp.bfloat16)
    low = (values - high.astype(jnp.float32)).astype(jnp.bfloat16)
    return high, low


def attention(
    tokens, norm_gain, query_w, key_w, value_w, forget_w, forget_bias,
    query_gain, key_gain, cache_key, cache_value, cache_gate, cache_len, out_w,
):
    seq_count = tokens.shape[0]
    heads_local = cache_gate.shape[1]
    kv_local = cache_key.shape[1]
    head_size = cache_key.shape[2]
    cache_span = cache_key.shape[3]
    tp_rank = lax.axis_index("tp")
    score_scale = head_size ** (-0.5)
    resid_in = tokens.astype(jnp.float32)
    normed = rms_scale(resid_in, norm_gain.astype(jnp.float32)).astype(jnp.bfloat16)
    queries = jnp.dot(normed, query_w, preferred_element_type=jnp.float32).reshape(
        seq_count, heads_local, head_size
    )
    queries = rms_scale(queries, query_gain.astype(jnp.float32)).astype(jnp.bfloat16)
    keys_all = jnp.dot(normed, key_w, preferred_element_type=jnp.float32).reshape(
        seq_count, -1, head_size
    )
    keys_all = rms_scale(keys_all, key_gain.astype(jnp.float32)).astype(jnp.bfloat16)
    values_all = (
        jnp.dot(normed, value_w, preferred_element_type=jnp.float32)
        .astype(jnp.bfloat16)
        .reshape(seq_count, -1, head_size)
    )
    fresh_key = lax.dynamic_slice_in_dim(keys_all, tp_rank * kv_local, kv_local, 1)
    fresh_value = lax.dynamic_slice_in_dim(values_all, tp_rank * kv_local, kv_local, 1)
    forget_all = jax.nn.log_sigmoid(
        jnp.dot(normed, forget_w, preferred_element_type=jnp.float32) + forget_bias
    )
    log_forget = lax.dynamic_slice_in_dim(forget_all, tp_rank * heads_local, heads_local, 1)
    repeat = heads_local // kv_local
    grouped = queries.reshape(seq_count, kv_local, repeat, head_size)
    scores = (
        jnp.einsum("sgrd,sgdl->sgrl", grouped, cache_key, preferred_element_type=jnp.float32)
        * score_scale
    )
    own_score = (
        jnp.einsum("sgrd,sgd->sgr", grouped, fresh_key, preferred_element_type=jnp.float32)
        * score_scale
    )
    slot = lax.broadcasted_iota(jnp.int32, (seq_count, cache_span), 1)
    at_last = (slot == cache_len[:, None] - 1)[:, None, :]
    previous = jnp.sum(jnp.where(at_last, cache_gate, jnp.zeros_like(cache_gate)), axis=2)
    current = previous + log_forget
    decay_bias = (current[:, :, None] - cache_gate).reshape(seq_count, kv_local, repeat, cache_span)
    is_valid = (slot < cache_len[:, None])[:, None, None, :]
    logits = jnp.where(is_valid, scores + decay_bias, -jnp.inf)
    top_logit = jnp.maximum(jnp.max(logits, axis=3), own_score)
    weights = jnp.exp(logits - top_logit[..., None])
    own_weight = jnp.exp(own_score - top_logit)
    total_weight = jnp.sum(weights, axis=3) + own_weight
    cache_probs = (weights / total_weight[..., None]).astype(jnp.bfloat16)
    own_prob = (own_weight / total_weight).astype(jnp.bfloat16)
    mixed_heads = jnp.einsum(
        "sgrl,sgdl->sgrd", cache_probs, cache_value, preferred_element_type=jnp.float32
    )
    mixed_heads = (
        mixed_heads
        + own_prob.astype(jnp.float32)[..., None] * fresh_value.astype(jnp.float32)[:, :, None, :]
    )
    attn_heads = mixed_heads.reshape(seq_count, heads_local * head_size).astype(jnp.bfloat16)
    partial = jnp.dot(attn_heads, out_w, preferred_element_type=jnp.float32).astype(jnp.bfloat16)
    return resid_in, partial, fresh_key, fresh_value, current


def route_slots(expert_choice, ep_count, capacity):
    route_ids = expert_choice.reshape(-1)
    member = (route_ids[:, None] == jnp.arange(ep_count)[None, :]).astype(jnp.float32)
    count = route_ids.shape[0]
    earlier = (
        lax.broadcasted_iota(jnp.int32, (count, count), 0)
        > lax.broadcasted_iota(jnp.int32, (count, count), 1)
    ).astype(jnp.float32)
    before = jnp.dot(earlier, member, preferred_element_type=jnp.float32)
    rank = jnp.sum(before * member, axis=1)
    slot = route_ids.astype(jnp.float32) * capacity + rank
    return slot.reshape(expert_choice.shape)


def body(
    tokens, norm_gain, query_w, key_w, value_w, forget_w, forget_bias, query_gain, key_gain,
    cache_key, cache_value, cache_gate, cache_len, out_w, post_gain, branch_gate,
    dense_gate_w, dense_up_w, dense_down_w, expert_choice, route_weight,
    expert_gate_w, expert_up_w, expert_down_w,
):
    f32, bf16 = jnp.float32, jnp.bfloat16
    seq, width = tokens.shape
    tp_count = lax.axis_size("tp")
    ep_count = lax.axis_size("ep")
    tp_rank = lax.axis_index("tp")
    ep_rank = lax.axis_index("ep")
    half = width // tp_count
    planes = GROUPS
    plane = ep_count // planes
    capacity = 2 * ((seq + 2 * plane - 1) // (2 * plane))
    top_k = expert_choice.shape[1]
    ff_total = dense_gate_w.shape[1] * ep_count * tp_count
    hidden_local = dense_gate_w.shape[1]

    def swap(values):
        return lax.ppermute(values, "tp", [(i, 1 - i) for i in range(tp_count)])

    def exchange(values, mask):
        return lax.ppermute(values, "ep", [(i, i ^ mask) for i in range(ep_count)])

    resid_in, partial, fresh_key, fresh_value, current = attention(
        tokens, norm_gain, query_w, key_w, value_w, forget_w, forget_bias,
        query_gain, key_gain, cache_key, cache_value, cache_gate, cache_len, out_w,
    )
    attn_sum = partial.astype(f32) + swap(partial).astype(f32)
    resid_out = (resid_in + attn_sum).astype(bf16).astype(f32)
    post_norm = rms_scale(resid_out, post_gain.astype(f32)).astype(bf16)

    slots = route_slots(expert_choice, ep_count, capacity)
    weight_high, weight_low = split_two(route_weight)
    notes = jnp.concatenate([slots.astype(bf16), weight_high, weight_low], axis=1)
    notes = jnp.pad(notes, ((0, 0), (0, LANES - notes.shape[1])))
    mine = lax.dynamic_slice_in_dim(post_norm, tp_rank * half, half, 1)
    payload = jnp.concatenate([mine, notes], axis=1)
    column = jnp.concatenate(
        [payload] + [exchange(payload, k * plane) for k in range(1, planes)], axis=0
    )
    gathered = jnp.concatenate(
        [column] + [exchange(column, j) for j in range(1, plane)], axis=0
    )
    rows_mine = gathered[:, :half]
    rows_other = swap(rows_mine)
    rows = jnp.where(
        tp_rank == 0,
        jnp.concatenate([rows_mine, rows_other], axis=1),
        jnp.concatenate([rows_other, rows_mine], axis=1),
    )
    info = gathered[:, half:].astype(f32)
    slot_of = info[:, :top_k].reshape(ep_count, seq, top_k)
    weight_of = (info[:, top_k : 2 * top_k] + info[:, 2 * top_k : 3 * top_k]).reshape(
        ep_count, seq, top_k
    )

    gate_value = jnp.dot(rows, dense_gate_w, preferred_element_type=f32)
    up_value = jnp.dot(rows, dense_up_w, preferred_element_type=f32)
    hidden = jax.nn.silu(gate_value) * up_value
    squares = jnp.sum(hidden * hidden, axis=1)
    dense = jnp.einsum(
        "sh,hcd->csd",
        hidden.astype(bf16),
        dense_down_w.reshape(hidden_local, tp_count, half),
        preferred_element_type=f32,
    )

    local_slot = (ep_rank * capacity + jnp.arange(capacity)).astype(f32)
    hit = (slot_of[:, None, :, :] == local_slot[None, :, None, None]).astype(f32)
    slot_weight = jnp.sum(hit * weight_of[:, None, :, :], axis=(2, 3)).reshape(-1)
    pick = jnp.sum(hit, axis=3).astype(bf16)
    same = jnp.eye(ep_count, dtype=bf16)
    pick_all = (pick[:, :, None, :] * same[:, None, :, None]).reshape(
        ep_count * capacity, ep_count * seq
    )
    slot_rows = jnp.dot(pick_all, rows, preferred_element_type=f32).astype(bf16)
    expert_gate = jnp.dot(slot_rows, expert_gate_w[0], preferred_element_type=f32)
    expert_up = jnp.dot(slot_rows, expert_up_w[0], preferred_element_type=f32)
    activated = (jax.nn.silu(expert_gate) * expert_up).astype(bf16)
    routed = jnp.einsum(
        "sh,hcd->csd",
        activated,
        expert_down_w[0].reshape(-1, tp_count, half),
        preferred_element_type=f32,
    )
    routed = routed * slot_weight[None, :, None]

    def pack(dense_part, routed_part, square_part):
        lead = square_part.shape[0]
        high, low = split_two(square_part.reshape(lead, 1, -1))
        extra = jnp.concatenate([high, low], axis=1)
        extra = jnp.pad(extra, ((0, 0), (0, 6), (0, half - extra.shape[2])))
        return jnp.concatenate(
            [
                dense_part.astype(bf16).reshape(lead, -1, half),
                routed_part.astype(bf16).reshape(lead, -1, half),
                extra,
            ],
            axis=1,
        )

    def unpack(values, dense_rows, routed_rows, square_count):
        values = values.astype(f32)
        base = dense_rows + routed_rows
        square_part = values[:, base, :square_count] + values[:, base + 1, :square_count]
        return values[:, :dense_rows], values[:, dense_rows:base], square_part

    def pick_half(values, index):
        return lax.dynamic_index_in_dim(values, index, 0, False)

    dense_rows = planes * seq
    routed_rows = planes * capacity
    sent = pack(
        pick_half(dense, 1 - tp_rank).reshape(plane, -1, half),
        pick_half(routed, 1 - tp_rank).reshape(plane, -1, half),
        squares.reshape(plane, -1),
    )
    dense_in, routed_in, squares_in = unpack(swap(sent), dense_rows, routed_rows, dense_rows)
    dense_chip = pick_half(dense, tp_rank).reshape(plane, dense_rows, half) + dense_in
    routed_chip = pick_half(routed, tp_rank).reshape(plane, routed_rows, half) + routed_in
    squares_chip = squares.reshape(plane, -1) + squares_in
    outgoing = pack(dense_chip, routed_chip, squares_chip)
    arrived = [exchange(outgoing[j], j) for j in range(1, plane)]
    arrived = jnp.stack([outgoing[0]] + arrived, axis=0)
    dense_a, routed_a, squares_a = unpack(arrived, dense_rows, routed_rows, dense_rows)
    dense_plane = jnp.sum(dense_a, axis=0).reshape(planes, seq, half)
    squares_plane = jnp.sum(squares_a, axis=0).reshape(planes, seq)

    z_rank = ep_rank // plane
    p_rank = ep_rank % plane
    peers = jnp.bitwise_xor(jnp.arange(plane), p_rank) + z_rank * plane
    peer_slot = (peers[:, None] * capacity + jnp.arange(capacity)[None, :]).astype(f32).reshape(-1)
    column_slot = slot_of.reshape(plane, planes, seq, top_k)[0]
    column_group = jnp.floor((column_slot[:, 0, 0] + 0.5) / (capacity * plane))
    own_plane = column_group == z_rank.astype(f32)
    pairs = column_slot.reshape(planes, seq // 2, 2, top_k)
    pairs = jnp.where(own_plane[:, None, None], pairs[:, :, 0], pairs[:, :, 1])
    combine = jnp.sum(
        (pairs[:, :, None, :] == peer_slot[None, None, :, None]).astype(f32), axis=3
    ).astype(bf16)
    routed_slots = arrived[:, dense_rows : dense_rows + routed_rows].reshape(
        plane, planes, capacity, half
    )
    routed_slots = jnp.transpose(routed_slots, (1, 0, 2, 3)).reshape(planes, plane * capacity, half)
    routed_plane = jnp.einsum("kts,ksd->ktd", combine, routed_slots, preferred_element_type=f32)

    last = pack(dense_plane, routed_plane, squares_plane)
    final = [exchange(last[k], k * plane) for k in range(1, planes)]
    final = jnp.stack([last[0]] + final, axis=0)
    half_seq = seq // 2
    dense_f, _, squares_f = unpack(final, seq, half_seq, seq)
    dense_sum = jnp.sum(dense_f, axis=0)
    square_sum = jnp.sum(squares_f, axis=0)
    my_group = column_group[0]
    z_peers = jnp.bitwise_xor(jnp.arange(planes), z_rank).astype(f32)
    parity = (z_peers != my_group).astype(jnp.int32)
    place = (
        jnp.arange(seq)[:, None, None]
        == 2 * jnp.arange(half_seq)[None, None, :] + parity[None, :, None]
    ).astype(bf16).reshape(seq, planes * half_seq)
    expert_sum = jnp.dot(
        place,
        final[:, seq : seq + half_seq].reshape(planes * half_seq, half),
        preferred_element_type=f32,
    )
    branch = jax.nn.sigmoid(jnp.dot(post_norm, branch_gate, preferred_element_type=f32))
    dense_out = dense_sum * lax.rsqrt(square_sum / ff_total + norm_eps)[:, None]
    resid_columns = lax.dynamic_slice_in_dim(resid_out, tp_rank * half, half, 1)
    mixed_out = (resid_columns + expert_sum + branch[:, None] * dense_out).astype(bf16)
    return (mixed_out, fresh_key, fresh_value, current)


def solution(mesh):
    placed = (
        P("ep", None), P(), P(None, "tp"), P(), P(), P(), P(), P(), P(),
        P("ep", "tp", None, None), P("ep", "tp", None, None), P("ep", "tp", None), P("ep"),
        P("tp", None), P(), P(),
        P(None, ("ep", "tp")), P(None, ("ep", "tp")), P(("ep", "tp"), None),
        P("ep", None), P("ep", None),
        P("ep", None, "tp"), P("ep", None, "tp"), P("ep", "tp", None),
    )
    return jax.shard_map(
        body,
        mesh=mesh,
        in_specs=placed,
        out_specs=(P("ep", "tp"), P("ep", "tp", None), P("ep", "tp", None), P("ep", "tp")),
        check_vma=False,
    )
```

```python
import functools

import jax
import jax.numpy as jnp
from jax import lax
from jax.experimental import pallas as pl
from jax.experimental.pallas import tpu as pltpu
from jax.sharding import PartitionSpec as P


GROUPS = 4
LANES = 128
BLOCK_KEY = 1024.0

norm_eps = 1e-06


def rms_scale(values, gain_vec):
    mean_square = jnp.mean(values * values, axis=-1, keepdims=True)
    return values * lax.rsqrt(mean_square + norm_eps) * gain_vec


def split_two(values):
    high = values.astype(jnp.bfloat16)
    low = (values - high.astype(jnp.float32)).astype(jnp.bfloat16)
    return high, low


def route_slots(expert_choice, ep_count, capacity):
    route_ids = expert_choice.reshape(-1)
    member = (route_ids[:, None] == jnp.arange(ep_count)[None, :]).astype(jnp.float32)
    count = route_ids.shape[0]
    earlier = (
        lax.broadcasted_iota(jnp.int32, (count, count), 0)
        > lax.broadcasted_iota(jnp.int32, (count, count), 1)
    ).astype(jnp.float32)
    before = jnp.dot(earlier, member, preferred_element_type=jnp.float32)
    rank = jnp.sum(before * member, axis=1)
    slot = route_ids.astype(jnp.float32) * capacity + rank
    return slot.reshape(expert_choice.shape)


F32, BF16 = jnp.float32, jnp.bfloat16
VMEM = pl.BlockSpec(memory_space=pltpu.VMEM)
SMEM = pl.BlockSpec(memory_space=pltpu.SMEM)


def call(kernel, outs, operands, hbm=(), scratch=(), limit=20):
    specs = []
    held = []
    for index, op in enumerate(operands):
        if index in hbm:
            specs.append(pl.BlockSpec(memory_space=pltpu.HBM))
            held.append(pltpu.with_memory_space_constraint(op, pltpu.HBM))
        elif op.dtype == jnp.int32 and op.ndim == 1:
            specs.append(SMEM)
            held.append(op)
        else:
            specs.append(VMEM)
            held.append(pltpu.with_memory_space_constraint(op, pltpu.VMEM))
    return pl.pallas_call(
        kernel,
        in_specs=specs,
        out_specs=[VMEM] * len(outs),
        out_shape=[pltpu.VMEM(shape, dtype) for shape, dtype in outs],
        scratch_shapes=list(scratch),
        compiler_params=pltpu.CompilerParams(vmem_limit_bytes=limit * 1024 * 1024),
    )(*held)


def axis_iota(shape, axis):
    return lax.broadcasted_iota(jnp.int32, shape, axis).astype(F32)


def block_of(index, size):
    return jnp.floor((index + 0.5) * (1.0 / size))


def dot(left, right):
    return jnp.dot(left, right, preferred_element_type=F32)


def high_low(values):
    high = values.astype(BF16).astype(F32)
    return high, values - high


def to_row(column):
    rows = column.shape[0]
    wide = jnp.broadcast_to(column, (rows, LANES))
    if rows < LANES:
        wide = jnp.concatenate([wide, jnp.zeros((LANES - rows, LANES), F32)], axis=0)
    return jnp.transpose(wide)[0:1]


def silu(values):
    return values / (1.0 + jnp.exp(-values))


def post_kernel(ids, tokens, part_a, part_b, gain, branch_gate, notes, payload, resid, branch):
    half = resid.shape[1]
    first = ids[0] == 0
    total = tokens[...].astype(F32) + (part_a[...].astype(F32) + part_b[...].astype(F32))
    total = total.astype(BF16).astype(F32)
    mean_square = jnp.mean(total * total, axis=-1, keepdims=True)
    post = (total * lax.rsqrt(mean_square + norm_eps) * gain[...].astype(F32)[None]).astype(BF16)
    gate = jnp.sum(post.astype(F32) * branch_gate[...].astype(F32)[None], axis=-1, keepdims=True)
    branch[...] = jnp.broadcast_to(1.0 / (1.0 + jnp.exp(-gate)), branch.shape)
    payload[:, :half] = jnp.where(first, post[:, :half], post[:, half:])
    payload[:, half:] = notes[...]
    resid[...] = jnp.where(first, total[:, :half], total[:, half:]).astype(BF16)


def load_kernel(
    ids, column, gate_in, up_in, expert_gate_in, expert_up_in, down_in, expert_in,
    combine, gate_w, up_w, expert_gate, expert_up, down_own, expert_own, down_sent, sems,
    *, seq, capacity, top_k,
):
    hidden, half = down_own.shape
    other = expert_own.shape[0]
    mine = pl.ds(pl.multiple_of(ids[0] * half, half), half)
    theirs = pl.ds(pl.multiple_of((1 - ids[0]) * half, half), half)
    pairs = [
        (down_in.at[:, theirs], down_sent.at[pl.ds(0, hidden)]),
        (expert_in.at[:, theirs], down_sent.at[pl.ds(hidden, other)]),
        (gate_in, gate_w), (up_in, up_w), (expert_gate_in, expert_gate),
        (expert_up_in, expert_up), (down_in.at[:, mine], down_own),
        (expert_in.at[:, mine], expert_own),
    ]
    copies = [pltpu.make_async_copy(a, b, sems.at[i]) for i, (a, b) in enumerate(pairs)]
    for copy in copies:
        copy.start()
    plane = combine.shape[0]
    planes = combine.shape[2] // capacity
    pair_rows = combine.shape[1] // planes
    tokens = planes * seq
    info = column[:, column.shape[1] - LANES :].astype(F32)
    near_key = block_of(axis_iota((tokens, 1), 0), seq) * BLOCK_KEY
    lane = axis_iota((1, planes * capacity), 1)
    lane_block = block_of(lane, capacity)
    lane_key = lane_block * BLOCK_KEY + (lane - lane_block * capacity)
    pair = axis_iota((planes * pair_rows, 1), 0)
    pair_block = block_of(pair, pair_rows)
    pair_offset = pair - pair_block * pair_rows
    pair_id = jnp.where(pair_offset < seq // 2, pair_block * (seq // 2) + pair_offset, -1.0)
    joined = (block_of(axis_iota((1, tokens), 1), 2) == pair_id).astype(BF16)
    for j in range(plane):
        match = jnp.zeros((tokens, planes * capacity), F32)
        for k in range(top_k):
            match = match + (
                info[:, k : k + 1] + near_key == lane_key + ids[2 + j].astype(F32)
            ).astype(F32)
        combine[j] = dot(joined, match.astype(BF16)).astype(BF16)
    for copy in copies:
        copy.wait()


def hidden_kernel(ids, *refs, seq, capacity, top_k):
    plane = (len(refs) - 9) // 2
    owns, others = refs[:plane], refs[plane : 2 * plane]
    gate_w, up_w, expert_gate, expert_up, out, slot_weight, lefts, rights, notes = refs[2 * plane :]
    count, half = lefts.shape
    slots = slot_weight.shape[0]
    group = count // plane
    for j in range(plane):
        rows = pl.ds(j * group, group)
        lefts[rows, :] = owns[j][:, :half]
        rights[rows, :] = others[j][:, :half]
        notes[rows, :] = owns[j][:, half:].astype(F32)
    own_rows = pl.ds(pl.multiple_of(ids[0] * half, half), half)
    other_rows = pl.ds(pl.multiple_of((1 - ids[0]) * half, half), half)
    left = lefts[...]
    right = rights[...]

    def project(rows_own, rows_other, weight):
        return dot(rows_own, weight[own_rows, :]) + dot(rows_other, weight[other_rows, :])

    hidden = silu(project(left, right, gate_w)) * project(left, right, up_w)
    out[0:count, 0 : gate_w.shape[1]] = hidden.astype(BF16)
    squares = jnp.sum(hidden * hidden, axis=1, keepdims=True)
    tile_row = lax.broadcasted_iota(jnp.int32, (2 * plane, LANES), 0)
    tile = jnp.zeros((2 * plane, LANES), F32)
    for j in range(plane):
        high, low = high_low(to_row(squares[j * group : (j + 1) * group]))
        tile = jnp.where(tile_row == 2 * j, high, jnp.where(tile_row == 2 * j + 1, low, tile))
    out[count + slots :, :] = jnp.zeros((2 * plane, out.shape[1]), BF16)
    out[count + slots :, 0:LANES] = tile.astype(BF16)

    turned = jnp.transpose(notes[...])
    token = axis_iota((1, count), 1)
    token_key = block_of(token, seq) * BLOCK_KEY
    slot = axis_iota((slots, 1), 0)
    slot_block = block_of(slot, capacity)
    slot_key = slot_block * BLOCK_KEY + (slot - slot_block * capacity) + ids[1].astype(F32)
    pick = jnp.zeros((slots, count), F32)
    weight = jnp.zeros((slots, count), F32)
    for k in range(top_k):
        hit = (turned[k : k + 1] + token_key == slot_key).astype(F32)
        value = turned[top_k + k : top_k + k + 1] + turned[2 * top_k + k : 2 * top_k + k + 1]
        pick = pick + hit
        weight = weight + hit * value
    slot_weight[...] = jnp.broadcast_to(
        jnp.sum(weight, axis=1, keepdims=True), slot_weight.shape
    )
    pick = pick.astype(BF16)
    rows_own = dot(pick, left).astype(BF16)
    rows_other = dot(pick, right).astype(BF16)
    active = silu(project(rows_own, rows_other, expert_gate)) * project(
        rows_own, rows_other, expert_up
    )
    out[count : count + slots, 0 : expert_gate.shape[1]] = active.astype(BF16)


def down_kernel(own, other, down_own, expert_own, down_got, slot_weight, *outs, count):
    plane = len(outs)
    half = outs[0].shape[1]
    slots = slot_weight.shape[0]
    hidden, routed_hidden = down_own.shape[0], expert_own.shape[0]
    dense = dot(own[0:count, 0:hidden], down_own[...]) + dot(
        other[0:count, 0:hidden], down_got[0:hidden, :]
    )
    routed_rows = slice(count, count + slots)
    routed = dot(own[routed_rows, 0:routed_hidden], expert_own[...]) + dot(
        other[routed_rows, 0:routed_hidden], down_got[hidden:, :]
    )
    routed = routed * slot_weight[:, 0:1]
    squares = own[count + slots :, 0:LANES].astype(F32) + other[count + slots :, 0:LANES].astype(F32)
    group, part = count // plane, slots // plane
    tile_row = lax.broadcasted_iota(jnp.int32, (8, LANES), 0)
    for j in range(plane):
        outs[j][0:group, :] = dense[j * group : (j + 1) * group].astype(BF16)
        outs[j][group : group + part, :] = routed[j * part : (j + 1) * part].astype(BF16)
        high, low = high_low(squares[2 * j : 2 * j + 1] + squares[2 * j + 1 : 2 * j + 2])
        outs[j][group + part :, :] = jnp.zeros((8, half), BF16)
        outs[j][group + part :, 0:LANES] = jnp.where(
            tile_row == 0, high, jnp.where(tile_row == 1, low, 0.0)
        ).astype(BF16)


def plane_kernel(*refs, planes, seq, capacity):
    plane = len(refs) - planes - 1
    parts, combine, outs = refs[:plane], refs[plane], refs[plane + 1 :]
    group, part = planes * seq, planes * capacity
    dense = parts[0][0:group, :].astype(F32)
    routed = dot(combine[0], parts[0][group : group + part, :])
    notes = parts[0][group + part :, 0:LANES].astype(F32)
    for j in range(1, plane):
        dense = dense + parts[j][0:group, :].astype(F32)
        routed = routed + dot(combine[j], parts[j][group : group + part, :])
        notes = notes + parts[j][group + part :, 0:LANES].astype(F32)
    high, low = high_low(notes[0:1] + notes[1:2])
    pair_rows = combine.shape[1] // planes
    tile_row = lax.broadcasted_iota(jnp.int32, (pair_rows, LANES), 0)
    for k in range(planes):
        outs[k][0:seq, :] = dense[k * seq : (k + 1) * seq].astype(BF16)
        tail = routed[k * pair_rows : (k + 1) * pair_rows]
        first = jnp.where(
            tile_row == seq // 2,
            high,
            jnp.where(tile_row == seq // 2 + 1, low, tail[:, 0:LANES]),
        )
        outs[k][seq:, 0:LANES] = first.astype(BF16)
        outs[k][seq:, LANES:] = tail[:, LANES:].astype(BF16)


def final_kernel(*refs, ff_total, route_base, top_k):
    planes = len(refs) - 5
    ids, parts = refs[0], refs[1 : 1 + planes]
    resid, branch, notes, out = refs[1 + planes :]
    seq = resid.shape[0]
    half_seq = seq // 2
    pair_rows = parts[0].shape[0] - seq
    group = block_of(notes[:, 0:1].astype(F32), route_base)
    token_pair = block_of(axis_iota((seq, 1), 0), 2)
    lane = axis_iota((1, pair_rows), 1)
    dense = jnp.zeros(out.shape, F32)
    routed = jnp.zeros(out.shape, F32)
    squares = jnp.zeros((seq, LANES), F32)
    for k in range(planes):
        dense = dense + parts[k][0:seq, :].astype(F32)
        tail = parts[k][seq:, :]
        place = jnp.where(
            (token_pair == lane) & (group == ids[k].astype(F32)), 1.0, 0.0
        ).astype(BF16)
        routed = routed + dot(place, tail)
        values = tail[:, 0:LANES].astype(F32)
        row = values[half_seq : half_seq + 1] + values[half_seq + 1 : half_seq + 2]
        turned = jnp.transpose(jnp.broadcast_to(row, (LANES, LANES)))
        squares = squares + turned[k * seq : (k + 1) * seq]
    scale = branch[:, 0:1] * lax.rsqrt(squares[:, 0:1] * (1.0 / ff_total) + norm_eps)
    out[...] = (resid[...].astype(F32) + routed + scale * dense).astype(BF16)


def attend_kernel(
    ids, lens, tokens_in, norm_in, query_in, key_in, bias_in,
    query_w, key_w, value_w, forget_w, cache_key, cache_value, cache_gate, out_w,
    partial, fresh_key, fresh_value, fresh_gate,
    q_w, k_w, v_w, f_w, keys, values, gates, o_w, q_rows, k_rows, v_rows, f_cols, g_cols, mixed,
    tokens, norm_gain, query_gain, key_gain, forget_bias, sems,
    *, heads, chunks,
):
    seq = tokens.shape[0]
    head = cache_key.shape[1]
    span = cache_key.shape[2]
    step = seq // chunks
    plain = [
        (tokens_in, tokens), (norm_in, norm_gain), (query_in, query_gain), (key_in, key_gain),
        (bias_in, forget_bias), (key_w, k_w), (value_w, v_w), (forget_w, f_w), (query_w, q_w),
    ]
    small = [pltpu.make_async_copy(a, b, sems.at[i]) for i, (a, b) in enumerate(plain)]
    base = len(small)
    parts = []
    for c in range(chunks):
        rows = pl.ds(c * step, step)
        for a, b in ((cache_key, keys), (cache_gate, gates), (cache_value, values)):
            parts.append(pltpu.make_async_copy(a.at[rows], b.at[rows], sems.at[base + len(parts)]))
    last = pltpu.make_async_copy(out_w, o_w, sems.at[base + len(parts)])
    for copy in small + parts + [last]:
        copy.start()
    for copy in small[:5]:
        copy.wait()
    small = small[5:]
    first = ids[0] == 0
    resid = tokens[...].astype(F32)
    mean_square = jnp.mean(resid * resid, axis=-1, keepdims=True)
    normed = (resid * lax.rsqrt(mean_square + norm_eps) * norm_gain[...].astype(F32)[None]).astype(BF16)
    small[0].wait()
    key = dot(normed, k_w[...])
    key = jnp.where(first, key[:, :head], key[:, head:])
    key = rms_scale(key, key_gain[...].astype(F32)[None]).astype(BF16)
    fresh_key[...] = key
    k_rows[...] = key.astype(F32)
    small[1].wait()
    value = dot(normed, v_w[...])
    value = jnp.where(first, value[:, :head], value[:, head:]).astype(BF16)
    fresh_value[...] = value
    v_rows[...] = value.astype(F32)
    small[2].wait()
    forget = lax.dot_general(
        normed, f_w[...], (((1,), (1,)), ((), ())), preferred_element_type=F32
    )
    forget = forget + forget_bias[...][None]
    forget = jnp.minimum(forget, 0.0) - jnp.log1p(jnp.exp(-jnp.abs(forget)))
    forget = jnp.where(first, forget[:, :heads], forget[:, heads:])
    wide = jnp.concatenate([forget, jnp.zeros((seq, LANES - heads), F32)], axis=1)
    wide = jnp.concatenate([wide, jnp.zeros((LANES - seq, LANES), F32)], axis=0)
    f_cols[...] = jnp.transpose(wide)[0:heads]
    small[3].wait()
    queries = dot(normed, q_w[...])
    for h in range(heads):
        part = queries[:, h * head : (h + 1) * head]
        part = rms_scale(part, query_gain[...].astype(F32)[None]).astype(BF16)
        q_rows[:, h, :] = part.astype(F32)
    g_cols[...] = jnp.zeros(g_cols.shape, F32)
    lane = lax.broadcasted_iota(jnp.int32, (heads, span), 1)
    lane_small = lax.broadcasted_iota(jnp.int32, (heads, LANES), 1)
    scale = head ** (-0.5)

    def one(s):
        length = lens[s]
        place = length - 1
        block = pl.multiple_of((place // LANES) * LANES, LANES)
        near = gates[s, :, pl.ds(block, LANES)]
        previous = jnp.sum(
            jnp.where(lane_small == place - block, near, 0.0), axis=1, keepdims=True
        )
        log_forget = f_cols[:, s : s + 1]
        current = previous + log_forget
        g_cols[:, s : s + 1] = current
        query = q_rows[s]
        own = jnp.sum(query * k_rows[s : s + 1], axis=1, keepdims=True) * scale
        logits = dot(query.astype(BF16), keys[s]) * scale + (current - gates[s])
        logits = jnp.where(lane < length, logits, -1e30)
        top = jnp.maximum(jnp.max(logits, axis=1, keepdims=True), own)
        weight = jnp.exp(logits - top)
        own_weight = jnp.exp(own - top)
        total = jnp.sum(weight, axis=1, keepdims=True) + own_weight
        inverse = 1.0 / total
        probs = (weight * inverse).astype(BF16)
        own_prob = (own_weight * inverse).astype(BF16).astype(F32)
        out = lax.dot_general(
            probs, values[s], (((1,), (1,)), ((), ())), preferred_element_type=F32
        )
        mixed[s] = out + own_prob * v_rows[s : s + 1]

    for c in range(chunks):
        for copy in parts[3 * c : 3 * c + 3]:
            copy.wait()
        for s in range(c * step, (c + 1) * step):
            one(s)
    turned = jnp.concatenate([g_cols[...], jnp.zeros((LANES - heads, LANES), F32)], axis=0)
    fresh_gate[...] = jnp.transpose(turned)[0:seq, 0:heads]
    last.wait()
    total = jnp.zeros(partial.shape, F32)
    for h in range(heads):
        total = total + dot(mixed[:, h, :].astype(BF16), o_w[h * head : (h + 1) * head, :])
    partial[...] = total.astype(BF16)


def attend(
    ids, tokens, norm_gain, query_w, key_w, value_w, forget_w, forget_bias,
    query_gain, key_gain, cache_key, cache_value, cache_gate, cache_len, out_w,
):
    seq, width = tokens.shape
    heads = cache_gate.shape[1]
    head, span = cache_key.shape[2:]
    chunks = 3 if seq % 3 == 0 else 1
    scratch = [
        pltpu.VMEM(query_w.shape, BF16), pltpu.VMEM(key_w.shape, BF16),
        pltpu.VMEM(value_w.shape, BF16), pltpu.VMEM(forget_w.shape[::-1], BF16),
        pltpu.VMEM((seq, head, span), BF16), pltpu.VMEM((seq, head, span), BF16),
        pltpu.VMEM((seq, heads, span), F32), pltpu.VMEM(out_w.shape, BF16),
        pltpu.VMEM((seq, heads, head), F32), pltpu.VMEM((seq, head), F32),
        pltpu.VMEM((seq, head), F32), pltpu.VMEM((heads, LANES), F32),
        pltpu.VMEM((heads, LANES), F32), pltpu.VMEM((seq, heads, head), F32),
        pltpu.VMEM(tokens.shape, BF16), pltpu.VMEM(norm_gain.shape, BF16),
        pltpu.VMEM(query_gain.shape, BF16), pltpu.VMEM(key_gain.shape, BF16),
        pltpu.VMEM(forget_bias.shape, F32),
        pltpu.SemaphoreType.DMA((10 + 3 * chunks,)),
    ]
    partial, fresh_key, fresh_value, current = call(
        functools.partial(attend_kernel, heads=heads, chunks=chunks),
        [((seq, width), BF16), ((seq, head), BF16), ((seq, head), BF16), ((seq, heads), F32)],
        [
            ids, cache_len, tokens, norm_gain, query_gain, key_gain, forget_bias, query_w, key_w, value_w, forget_w.T,
            cache_key[:, 0], cache_value[:, 0], cache_gate, out_w,
        ],
        hbm=range(2, 15),
        scratch=scratch,
        limit=32,
    )
    return partial, fresh_key[:, None], fresh_value[:, None], current


def body(
    tokens, norm_gain, query_w, key_w, value_w, forget_w, forget_bias, query_gain, key_gain,
    cache_key, cache_value, cache_gate, cache_len, out_w, post_gain, branch_gate,
    dense_gate_w, dense_up_w, dense_down_w, expert_choice, route_weight,
    expert_gate_w, expert_up_w, expert_down_w,
):
    seq, width = tokens.shape
    tp_count = lax.axis_size("tp")
    ep_count = lax.axis_size("ep")
    tp_rank = lax.axis_index("tp")
    ep_rank = lax.axis_index("ep")
    half = width // tp_count
    planes = GROUPS
    plane = ep_count // planes
    capacity = 2 * ((seq + 2 * plane - 1) // (2 * plane))
    top_k = expert_choice.shape[1]
    ff_local = dense_gate_w.shape[1]
    expert_local = expert_gate_w.shape[2]
    widest = max(ff_local, expert_local)
    ff_total = ff_local * ep_count * tp_count
    count, slots = ep_count * seq, ep_count * capacity
    pair_rows = 8 * ((seq // 2 + 2 + 7) // 8)
    z_rank = ep_rank // plane
    p_rank = ep_rank % plane

    def swap(values):
        return lax.ppermute(values, "tp", [(i, 1 - i) for i in range(tp_count)])

    def exchange(values, mask):
        return lax.ppermute(values, "ep", [(i, i ^ mask) for i in range(ep_count)])

    slot_ids = route_slots(expert_choice, ep_count, capacity)
    weight_high, weight_low = split_two(route_weight)
    notes = jnp.concatenate([slot_ids.astype(BF16), weight_high, weight_low], axis=1)
    notes = jnp.pad(notes, ((0, 0), (0, LANES - notes.shape[1])))
    peers = jnp.bitwise_xor(jnp.arange(plane, dtype=jnp.int32), p_rank) + z_rank * plane
    ids = jnp.concatenate([jnp.stack([tp_rank, ep_rank * capacity]), peers * capacity])
    ids = ids.astype(jnp.int32)
    z_peers = jnp.bitwise_xor(jnp.arange(planes, dtype=jnp.int32), z_rank)

    partial, fresh_key, fresh_value, current = attend(
        ids, tokens, norm_gain, query_w, key_w, value_w, forget_w, forget_bias,
        query_gain, key_gain, cache_key, cache_value, cache_gate, cache_len, out_w,
    )
    payload, resid, branch = call(
        post_kernel,
        [((seq, half + LANES), BF16), ((seq, half), BF16), ((seq, LANES), F32)],
        [ids, tokens, partial, swap(partial), post_gain, branch_gate, notes],
    )
    column = jnp.concatenate(
        [payload] + [exchange(payload, k * plane) for k in range(1, planes)], axis=0
    )
    owns = [column] + [None] * (plane - 1)
    for j in reversed(range(1, plane)):
        owns[j] = exchange(column, j)
    combine, gate_w, up_w, expert_gate, expert_up, down_own, expert_own, down_sent = call(
        functools.partial(load_kernel, seq=seq, capacity=capacity, top_k=top_k),
        [((plane, planes * pair_rows, planes * capacity), BF16)]
        + [(dense_gate_w.shape, BF16)] * 2
        + [(expert_gate_w.shape[1:], BF16)] * 2
        + [((ff_local, half), BF16), ((expert_local, half), BF16)]
        + [((ff_local + expert_local, half), BF16)],
        [
            ids, column, dense_gate_w, dense_up_w, expert_gate_w[0], expert_up_w[0],
            dense_down_w, expert_down_w[0],
        ],
        hbm=range(2, 8),
        scratch=[pltpu.SemaphoreType.DMA((8,))],
    )
    down_got = swap(down_sent)
    others = [swap(values) for values in owns]
    hidden, slot_weight = call(
        functools.partial(hidden_kernel, seq=seq, capacity=capacity, top_k=top_k),
        [((count + slots + 2 * plane, widest), BF16), ((slots, LANES), F32)],
        [ids, *owns, *others, gate_w, up_w, expert_gate, expert_up],
        scratch=[
            pltpu.VMEM((count, half), BF16), pltpu.VMEM((count, half), BF16),
            pltpu.VMEM((count, LANES), F32),
        ],
    )
    sums = call(
        functools.partial(down_kernel, count=count),
        [((planes * (seq + capacity) + 8, half), BF16)] * plane,
        [
            hidden, swap(hidden), down_own, expert_own, down_got, slot_weight,
        ],
    )
    arrived = [sums[0]] + [None] * (plane - 1)
    for j in reversed(range(1, plane)):
        arrived[j] = exchange(sums[j], j)
    lasts = call(
        functools.partial(plane_kernel, planes=planes, seq=seq, capacity=capacity),
        [((seq + pair_rows, half), BF16)] * planes,
        [*arrived, combine],
    )
    final = [lasts[0]] + [exchange(lasts[k], k * plane) for k in range(1, planes)]
    (mixed_out,) = call(
        functools.partial(
            final_kernel, ff_total=ff_total, route_base=capacity * plane, top_k=top_k
        ),
        [((seq, half), BF16)],
        [z_peers, *final, resid, branch, notes],
    )
    return (mixed_out, fresh_key, fresh_value, current)


def solution(mesh):
    placed = (
        P("ep", None), P(), P(None, "tp"), P(), P(), P(), P(), P(), P(),
        P("ep", "tp", None, None), P("ep", "tp", None, None), P("ep", "tp", None), P("ep"),
        P("tp", None), P(), P(),
        P(None, ("ep", "tp")), P(None, ("ep", "tp")), P(("ep", "tp"), None),
        P("ep", None), P("ep", None),
        P("ep", None, "tp"), P("ep", None, "tp"), P("ep", "tp", None),
    )
    return jax.shard_map(
        body,
        mesh=mesh,
        in_specs=placed,
        out_specs=(P("ep", "tp"), P("ep", "tp", None), P("ep", "tp", None), P("ep", "tp")),
        check_vma=False,
    )
```

```python
import functools

import jax
import jax.numpy as jnp
from jax import lax
from jax.experimental import pallas as pl
from jax.experimental.pallas import tpu as pltpu
from jax.sharding import PartitionSpec as P


GROUPS = 4
LANES = 128
BLOCK_KEY = 1024.0

norm_eps = 1e-06


def rms_scale(values, gain_vec):
    mean_square = jnp.mean(values * values, axis=-1, keepdims=True)
    return values * lax.rsqrt(mean_square + norm_eps) * gain_vec


def split_two(values):
    high = values.astype(jnp.bfloat16)
    low = (values - high.astype(jnp.float32)).astype(jnp.bfloat16)
    return high, low


def route_slots(expert_choice, ep_count, capacity):
    route_ids = expert_choice.reshape(-1)
    member = (route_ids[:, None] == jnp.arange(ep_count)[None, :]).astype(jnp.float32)
    count = route_ids.shape[0]
    earlier = (
        lax.broadcasted_iota(jnp.int32, (count, count), 0)
        > lax.broadcasted_iota(jnp.int32, (count, count), 1)
    ).astype(jnp.float32)
    before = jnp.dot(earlier, member, preferred_element_type=jnp.float32)
    rank = jnp.sum(before * member, axis=1)
    slot = route_ids.astype(jnp.float32) * capacity + rank
    return slot.reshape(expert_choice.shape)


F32, BF16 = jnp.float32, jnp.bfloat16
VMEM = pl.BlockSpec(memory_space=pltpu.VMEM)
SMEM = pl.BlockSpec(memory_space=pltpu.SMEM)


def call(kernel, outs, operands, hbm=(), scratch=(), limit=20):
    specs = []
    held = []
    for index, op in enumerate(operands):
        if index in hbm:
            specs.append(pl.BlockSpec(memory_space=pltpu.HBM))
            held.append(pltpu.with_memory_space_constraint(op, pltpu.HBM))
        elif op.dtype == jnp.int32 and op.ndim == 1:
            specs.append(SMEM)
            held.append(op)
        else:
            specs.append(VMEM)
            held.append(pltpu.with_memory_space_constraint(op, pltpu.VMEM))
    return pl.pallas_call(
        kernel,
        in_specs=specs,
        out_specs=[VMEM] * len(outs),
        out_shape=[pltpu.VMEM(shape, dtype) for shape, dtype in outs],
        scratch_shapes=list(scratch),
        compiler_params=pltpu.CompilerParams(vmem_limit_bytes=limit * 1024 * 1024),
    )(*held)


def axis_iota(shape, axis):
    return lax.broadcasted_iota(jnp.int32, shape, axis).astype(F32)


def block_of(index, size):
    return jnp.floor((index + 0.5) * (1.0 / size))


def dot(left, right):
    return jnp.dot(left, right, preferred_element_type=F32)


def high_low(values):
    high = values.astype(BF16).astype(F32)
    return high, values - high


def to_row(column):
    rows = column.shape[0]
    wide = jnp.broadcast_to(column, (rows, LANES))
    if rows < LANES:
        wide = jnp.concatenate([wide, jnp.zeros((LANES - rows, LANES), F32)], axis=0)
    return jnp.transpose(wide)[0:1]


def silu(values):
    return values / (1.0 + jnp.exp(-values))


def post_kernel(ids, tokens, part_a, part_b, gain, branch_gate, notes, payload, resid, branch):
    half = resid.shape[1]
    first = ids[0] == 0
    total = tokens[...].astype(F32) + (part_a[...].astype(F32) + part_b[...].astype(F32))
    total = total.astype(BF16).astype(F32)
    mean_square = jnp.mean(total * total, axis=-1, keepdims=True)
    post = (total * lax.rsqrt(mean_square + norm_eps) * gain[...].astype(F32)[None]).astype(BF16)
    gate = jnp.sum(post.astype(F32) * branch_gate[...].astype(F32)[None], axis=-1, keepdims=True)
    branch[...] = jnp.broadcast_to(1.0 / (1.0 + jnp.exp(-gate)), branch.shape)
    payload[:, :half] = jnp.where(first, post[:, :half], post[:, half:])
    payload[:, half:] = notes[...]
    resid[...] = jnp.where(first, total[:, :half], total[:, half:]).astype(BF16)


def fetch_kernel(anchor, *refs):
    count = (len(refs) - 1) // 2
    copies = [
        pltpu.make_async_copy(refs[i], refs[count + i], refs[-1].at[i]) for i in range(count)
    ]
    for copy in copies:
        copy.start()
    for copy in copies:
        copy.wait()


def load_kernel(
    ids, column, down_in, expert_in, combine, down_own, expert_own, down_sent, sems,
    *, seq, capacity, top_k,
):
    hidden, half = down_own.shape
    other = expert_own.shape[0]
    mine = pl.ds(pl.multiple_of(ids[0] * half, half), half)
    theirs = pl.ds(pl.multiple_of((1 - ids[0]) * half, half), half)
    pairs = [
        (down_in.at[:, theirs], down_sent.at[pl.ds(0, hidden)]),
        (expert_in.at[:, theirs], down_sent.at[pl.ds(hidden, other)]),
        (down_in.at[:, mine], down_own),
        (expert_in.at[:, mine], expert_own),
    ]
    copies = [pltpu.make_async_copy(a, b, sems.at[i]) for i, (a, b) in enumerate(pairs)]
    for copy in copies:
        copy.start()
    plane = combine.shape[0]
    planes = combine.shape[2] // capacity
    pair_rows = combine.shape[1] // planes
    tokens = planes * seq
    info = column[:, column.shape[1] - LANES :].astype(F32)
    near_key = block_of(axis_iota((tokens, 1), 0), seq) * BLOCK_KEY
    lane = axis_iota((1, planes * capacity), 1)
    lane_block = block_of(lane, capacity)
    lane_key = lane_block * BLOCK_KEY + (lane - lane_block * capacity)
    pair = axis_iota((planes * pair_rows, 1), 0)
    pair_block = block_of(pair, pair_rows)
    pair_offset = pair - pair_block * pair_rows
    pair_id = jnp.where(pair_offset < seq // 2, pair_block * (seq // 2) + pair_offset, -1.0)
    joined = (block_of(axis_iota((1, tokens), 1), 2) == pair_id).astype(BF16)
    for j in range(plane):
        match = jnp.zeros((tokens, planes * capacity), F32)
        for k in range(top_k):
            match = match + (
                info[:, k : k + 1] + near_key == lane_key + ids[2 + j].astype(F32)
            ).astype(F32)
        combine[j] = dot(joined, match.astype(BF16)).astype(BF16)
    for copy in copies:
        copy.wait()


def hidden_kernel(ids, *refs, seq, capacity, top_k):
    plane = (len(refs) - 9) // 2
    owns, others = refs[:plane], refs[plane : 2 * plane]
    gate_w, up_w, expert_gate, expert_up, out, slot_weight, lefts, rights, notes = refs[2 * plane :]
    count, half = lefts.shape
    slots = slot_weight.shape[0]
    group = count // plane
    for j in range(plane):
        rows = pl.ds(j * group, group)
        lefts[rows, :] = owns[j][:, :half]
        rights[rows, :] = others[j][:, :half]
        notes[rows, :] = owns[j][:, half:].astype(F32)
    own_rows = pl.ds(pl.multiple_of(ids[0] * half, half), half)
    other_rows = pl.ds(pl.multiple_of((1 - ids[0]) * half, half), half)
    left = lefts[...]
    right = rights[...]

    def project(rows_own, rows_other, weight):
        return dot(rows_own, weight[own_rows, :]) + dot(rows_other, weight[other_rows, :])

    hidden = silu(project(left, right, gate_w)) * project(left, right, up_w)
    out[0:count, 0 : gate_w.shape[1]] = hidden.astype(BF16)
    squares = jnp.sum(hidden * hidden, axis=1, keepdims=True)
    extra = out.shape[0] - count - slots
    tile_row = lax.broadcasted_iota(jnp.int32, (extra, LANES), 0)
    tile = jnp.zeros((extra, LANES), F32)
    for j in range(plane):
        high, low = high_low(to_row(squares[j * group : (j + 1) * group]))
        tile = jnp.where(tile_row == 2 * j, high, jnp.where(tile_row == 2 * j + 1, low, tile))
    out[count + slots :, :] = jnp.zeros((extra, out.shape[1]), BF16)
    out[count + slots :, 0:LANES] = tile.astype(BF16)

    turned = jnp.transpose(notes[...])
    token = axis_iota((1, count), 1)
    token_key = block_of(token, seq) * BLOCK_KEY
    slot = axis_iota((slots, 1), 0)
    slot_block = block_of(slot, capacity)
    slot_key = slot_block * BLOCK_KEY + (slot - slot_block * capacity) + ids[1].astype(F32)
    pick = jnp.zeros((slots, count), F32)
    weight = jnp.zeros((slots, count), F32)
    for k in range(top_k):
        hit = (turned[k : k + 1] + token_key == slot_key).astype(F32)
        value = turned[top_k + k : top_k + k + 1] + turned[2 * top_k + k : 2 * top_k + k + 1]
        pick = pick + hit
        weight = weight + hit * value
    slot_weight[...] = jnp.broadcast_to(
        jnp.sum(weight, axis=1, keepdims=True), slot_weight.shape
    )
    pick = pick.astype(BF16)
    rows_own = dot(pick, left).astype(BF16)
    rows_other = dot(pick, right).astype(BF16)
    active = silu(project(rows_own, rows_other, expert_gate)) * project(
        rows_own, rows_other, expert_up
    )
    out[count : count + slots, 0 : expert_gate.shape[1]] = active.astype(BF16)


def down_kernel(own, other, down_own, expert_own, down_got, slot_weight, *outs, count):
    plane = len(outs)
    half = outs[0].shape[1]
    slots = slot_weight.shape[0]
    hidden, routed_hidden = down_own.shape[0], expert_own.shape[0]
    dense = dot(own[0:count, 0:hidden], down_own[...]) + dot(
        other[0:count, 0:hidden], down_got[0:hidden, :]
    )
    routed_rows = slice(count, count + slots)
    routed = dot(own[routed_rows, 0:routed_hidden], expert_own[...]) + dot(
        other[routed_rows, 0:routed_hidden], down_got[hidden:, :]
    )
    routed = routed * slot_weight[:, 0:1]
    squares = own[count + slots :, 0:LANES].astype(F32) + other[count + slots :, 0:LANES].astype(F32)
    group, part = count // plane, slots // plane
    tile_row = lax.broadcasted_iota(jnp.int32, (8, LANES), 0)
    for j in range(plane):
        outs[j][0:group, :] = dense[j * group : (j + 1) * group].astype(BF16)
        outs[j][group : group + part, :] = routed[j * part : (j + 1) * part].astype(BF16)
        high, low = high_low(squares[2 * j : 2 * j + 1] + squares[2 * j + 1 : 2 * j + 2])
        outs[j][group + part :, :] = jnp.zeros((8, half), BF16)
        outs[j][group + part :, 0:LANES] = jnp.where(
            tile_row == 0, high, jnp.where(tile_row == 1, low, 0.0)
        ).astype(BF16)


def plane_kernel(*refs, planes, seq, capacity):
    plane = len(refs) - planes - 1
    parts, combine, outs = refs[:plane], refs[plane], refs[plane + 1 :]
    group, part = planes * seq, planes * capacity
    dense = parts[0][0:group, :].astype(F32)
    routed = dot(combine[0], parts[0][group : group + part, :])
    notes = parts[0][group + part :, 0:LANES].astype(F32)
    for j in range(1, plane):
        dense = dense + parts[j][0:group, :].astype(F32)
        routed = routed + dot(combine[j], parts[j][group : group + part, :])
        notes = notes + parts[j][group + part :, 0:LANES].astype(F32)
    high, low = high_low(notes[0:1] + notes[1:2])
    pair_rows = combine.shape[1] // planes
    tile_row = lax.broadcasted_iota(jnp.int32, (pair_rows, LANES), 0)
    for k in range(planes):
        outs[k][0:seq, :] = dense[k * seq : (k + 1) * seq].astype(BF16)
        tail = routed[k * pair_rows : (k + 1) * pair_rows]
        first = jnp.where(
            tile_row == seq // 2,
            high,
            jnp.where(tile_row == seq // 2 + 1, low, tail[:, 0:LANES]),
        )
        outs[k][seq:, 0:LANES] = first.astype(BF16)
        outs[k][seq:, LANES:] = tail[:, LANES:].astype(BF16)


def final_kernel(*refs, ff_total, route_base, top_k):
    planes = len(refs) - 5
    ids, parts = refs[0], refs[1 : 1 + planes]
    resid, branch, notes, out = refs[1 + planes :]
    seq = resid.shape[0]
    half_seq = seq // 2
    pair_rows = parts[0].shape[0] - seq
    group = block_of(notes[:, 0:1].astype(F32), route_base)
    token_pair = block_of(axis_iota((seq, 1), 0), 2)
    lane = axis_iota((1, pair_rows), 1)
    dense = jnp.zeros(out.shape, F32)
    routed = jnp.zeros(out.shape, F32)
    squares = jnp.zeros((seq, LANES), F32)
    for k in range(planes):
        dense = dense + parts[k][0:seq, :].astype(F32)
        tail = parts[k][seq:, :]
        place = jnp.where(
            (token_pair == lane) & (group == ids[k].astype(F32)), 1.0, 0.0
        ).astype(BF16)
        routed = routed + dot(place, tail)
        values = tail[:, 0:LANES].astype(F32)
        row = values[half_seq : half_seq + 1] + values[half_seq + 1 : half_seq + 2]
        turned = jnp.transpose(jnp.broadcast_to(row, (LANES, LANES)))
        squares = squares + turned[k * seq : (k + 1) * seq]
    scale = branch[:, 0:1] * lax.rsqrt(squares[:, 0:1] * (1.0 / ff_total) + norm_eps)
    out[...] = (resid[...].astype(F32) + routed + scale * dense).astype(BF16)


def attend_kernel(
    ids, lens_in, tokens_in, norm_in, query_in, key_in, bias_in,
    query_w, key_w, value_w, forget_w, cache_key, cache_value, cache_gate, out_w,
    partial, fresh_key, fresh_value, fresh_gate,
    q_w, k_w, v_w, f_w, keys, values, gates, o_w, q_rows, k_rows, v_rows, f_cols, g_cols, mixed,
    tokens, norm_gain, query_gain, key_gain, forget_bias, lens, sems,
    *, heads, chunks,
):
    seq = tokens.shape[0]
    head = cache_key.shape[1]
    span = cache_key.shape[2]
    step = seq // chunks
    plain = [
        (tokens_in, tokens), (norm_in, norm_gain), (query_in, query_gain), (key_in, key_gain),
        (bias_in, forget_bias), (lens_in, lens), (key_w, k_w), (value_w, v_w), (forget_w, f_w), (query_w, q_w),
    ]
    small = [pltpu.make_async_copy(a, b, sems.at[i]) for i, (a, b) in enumerate(plain)]
    base = len(small)
    parts = []
    for c in range(chunks):
        rows = pl.ds(c * step, step)
        for a, b in ((cache_key, keys), (cache_gate, gates), (cache_value, values)):
            parts.append(pltpu.make_async_copy(a.at[rows], b.at[rows], sems.at[base + len(parts)]))
    last = pltpu.make_async_copy(out_w, o_w, sems.at[base + len(parts)])
    for copy in small + parts + [last]:
        copy.start()
    for copy in small[:6]:
        copy.wait()
    small = small[6:]
    first = ids[0] == 0
    resid = tokens[...].astype(F32)
    mean_square = jnp.mean(resid * resid, axis=-1, keepdims=True)
    normed = (resid * lax.rsqrt(mean_square + norm_eps) * norm_gain[...].astype(F32)[None]).astype(BF16)
    small[0].wait()
    key = dot(normed, k_w[...])
    key = jnp.where(first, key[:, :head], key[:, head:])
    key = rms_scale(key, key_gain[...].astype(F32)[None]).astype(BF16)
    fresh_key[...] = key
    k_rows[...] = key.astype(F32)
    small[1].wait()
    value = dot(normed, v_w[...])
    value = jnp.where(first, value[:, :head], value[:, head:]).astype(BF16)
    fresh_value[...] = value
    v_rows[...] = value.astype(F32)
    small[2].wait()
    forget = lax.dot_general(
        normed, f_w[...], (((1,), (1,)), ((), ())), preferred_element_type=F32
    )
    forget = forget + forget_bias[...][None]
    forget = jnp.minimum(forget, 0.0) - jnp.log1p(jnp.exp(-jnp.abs(forget)))
    forget = jnp.where(first, forget[:, :heads], forget[:, heads:])
    wide = jnp.concatenate([forget, jnp.zeros((seq, LANES - heads), F32)], axis=1)
    wide = jnp.concatenate([wide, jnp.zeros((LANES - seq, LANES), F32)], axis=0)
    f_cols[...] = jnp.transpose(wide)[0:heads]
    small[3].wait()
    queries = dot(normed, q_w[...])
    scale = head ** (-0.5)
    for h in range(heads):
        part = queries[:, h * head : (h + 1) * head]
        part = rms_scale(part, query_gain[...].astype(F32)[None]).astype(BF16)
        q_rows[:, h, :] = part.astype(F32) * scale
    g_cols[...] = jnp.zeros(g_cols.shape, F32)
    lane = lax.broadcasted_iota(jnp.int32, (heads, span), 1)
    lane_small = lax.broadcasted_iota(jnp.int32, (heads, LANES), 1)

    def several(span_of):
        lengths = [lens[s] for s in span_of]
        place = [length - 1 for length in lengths]
        block = [pl.multiple_of((at // LANES) * LANES, LANES) for at in place]
        near = [gates[s, :, pl.ds(at, LANES)] for s, at in zip(span_of, block)]
        previous = [
            jnp.sum(jnp.where(lane_small == at - start, value, 0.0), axis=1, keepdims=True)
            for at, start, value in zip(place, block, near)
        ]
        current = [f_cols[:, s : s + 1] + value for s, value in zip(span_of, previous)]
        for s, value in zip(span_of, current):
            g_cols[:, s : s + 1] = value
        query = [q_rows[s] for s in span_of]
        scores = [dot(value.astype(BF16), keys[s]) for s, value in zip(span_of, query)]
        own = [
            jnp.sum(value * k_rows[s : s + 1], axis=1, keepdims=True)
            for s, value in zip(span_of, query)
        ]
        logits = [
            jnp.where(lane < length, score + (now - gates[s]), -1e30)
            for s, length, score, now in zip(span_of, lengths, scores, current)
        ]
        top = [
            jnp.maximum(jnp.max(value, axis=1, keepdims=True), mine)
            for value, mine in zip(logits, own)
        ]
        weight = [jnp.exp(value - peak) for value, peak in zip(logits, top)]
        own_weight = [jnp.exp(mine - peak) for mine, peak in zip(own, top)]
        inverse = [
            1.0 / (jnp.sum(value, axis=1, keepdims=True) + mine)
            for value, mine in zip(weight, own_weight)
        ]
        probs = [(value * factor).astype(BF16) for value, factor in zip(weight, inverse)]
        out = [
            lax.dot_general(
                value, values[s], (((1,), (1,)), ((), ())), preferred_element_type=F32
            )
            for s, value in zip(span_of, probs)
        ]
        for s, value, mine, factor in zip(span_of, out, own_weight, inverse):
            own_prob = (mine * factor).astype(BF16).astype(F32)
            mixed[s] = value + own_prob * v_rows[s : s + 1]

    for c in range(chunks):
        for copy in parts[3 * c : 3 * c + 3]:
            copy.wait()
        for start in range(c * step, (c + 1) * step, 12):
            several(range(start, min(start + 12, (c + 1) * step)))
    turned = jnp.concatenate([g_cols[...], jnp.zeros((LANES - heads, LANES), F32)], axis=0)
    fresh_gate[...] = jnp.transpose(turned)[0:seq, 0:heads]
    last.wait()
    total = jnp.zeros(partial.shape, F32)
    for h in range(heads):
        total = total + dot(mixed[:, h, :].astype(BF16), o_w[h * head : (h + 1) * head, :])
    partial[...] = total.astype(BF16)


def attend(
    ids, tokens, norm_gain, query_w, key_w, value_w, forget_w, forget_bias,
    query_gain, key_gain, cache_key, cache_value, cache_gate, cache_len, out_w,
):
    seq, width = tokens.shape
    heads = cache_gate.shape[1]
    head, span = cache_key.shape[2:]
    chunks = 2 if seq % 2 == 0 else 1
    scratch = [
        pltpu.VMEM(query_w.shape, BF16), pltpu.VMEM(key_w.shape, BF16),
        pltpu.VMEM(value_w.shape, BF16), pltpu.VMEM(forget_w.shape[::-1], BF16),
        pltpu.VMEM((seq, head, span), BF16), pltpu.VMEM((seq, head, span), BF16),
        pltpu.VMEM((seq, heads, span), F32), pltpu.VMEM(out_w.shape, BF16),
        pltpu.VMEM((seq, heads, head), F32), pltpu.VMEM((seq, head), F32),
        pltpu.VMEM((seq, head), F32), pltpu.VMEM((heads, LANES), F32),
        pltpu.VMEM((heads, LANES), F32), pltpu.VMEM((seq, heads, head), F32),
        pltpu.VMEM(tokens.shape, BF16), pltpu.VMEM(norm_gain.shape, BF16),
        pltpu.VMEM(query_gain.shape, BF16), pltpu.VMEM(key_gain.shape, BF16),
        pltpu.VMEM(forget_bias.shape, F32), pltpu.SMEM(cache_len.shape, jnp.int32),
        pltpu.SemaphoreType.DMA((11 + 3 * chunks,)),
    ]
    partial, fresh_key, fresh_value, current = call(
        functools.partial(attend_kernel, heads=heads, chunks=chunks),
        [((seq, width), BF16), ((seq, head), BF16), ((seq, head), BF16), ((seq, heads), F32)],
        [
            ids, cache_len, tokens, norm_gain, query_gain, key_gain, forget_bias, query_w, key_w, value_w, forget_w.T,
            cache_key[:, 0], cache_value[:, 0], cache_gate, out_w,
        ],
        hbm=range(1, 15),
        scratch=scratch,
        limit=32,
    )
    return partial, fresh_key[:, None], fresh_value[:, None], current


def body(
    tokens, norm_gain, query_w, key_w, value_w, forget_w, forget_bias, query_gain, key_gain,
    cache_key, cache_value, cache_gate, cache_len, out_w, post_gain, branch_gate,
    dense_gate_w, dense_up_w, dense_down_w, expert_choice, route_weight,
    expert_gate_w, expert_up_w, expert_down_w,
):
    seq, width = tokens.shape
    tp_count = lax.axis_size("tp")
    ep_count = lax.axis_size("ep")
    tp_rank = lax.axis_index("tp")
    ep_rank = lax.axis_index("ep")
    half = width // tp_count
    planes = GROUPS
    plane = ep_count // planes
    capacity = 2 * ((seq + 2 * plane - 1) // (2 * plane))
    top_k = expert_choice.shape[1]
    ff_local = dense_gate_w.shape[1]
    expert_local = expert_gate_w.shape[2]
    widest = max(ff_local, expert_local)
    ff_total = ff_local * ep_count * tp_count
    pair_rows = 8 * ((seq // 2 + 2 + 7) // 8)
    z_rank = ep_rank // plane
    p_rank = ep_rank % plane

    def swap(values):
        return lax.ppermute(values, "tp", [(i, 1 - i) for i in range(tp_count)])

    def exchange(values, mask):
        return lax.ppermute(values, "ep", [(i, i ^ mask) for i in range(ep_count)])

    slot_ids = route_slots(expert_choice, ep_count, capacity)
    weight_high, weight_low = split_two(route_weight)
    notes = jnp.concatenate([slot_ids.astype(BF16), weight_high, weight_low], axis=1)
    notes = jnp.pad(notes, ((0, 0), (0, LANES - notes.shape[1])))
    peers = jnp.bitwise_xor(jnp.arange(plane, dtype=jnp.int32), p_rank) + z_rank * plane
    ids = jnp.concatenate([jnp.stack([tp_rank, ep_rank * capacity]), peers * capacity])
    ids = ids.astype(jnp.int32)
    z_peers = jnp.bitwise_xor(jnp.arange(planes, dtype=jnp.int32), z_rank)

    partial, fresh_key, fresh_value, current = attend(
        ids, tokens, norm_gain, query_w, key_w, value_w, forget_w, forget_bias,
        query_gain, key_gain, cache_key, cache_value, cache_gate, cache_len, out_w,
    )
    payload, resid, branch = call(
        post_kernel,
        [((seq, half + LANES), BF16), ((seq, half), BF16), ((seq, LANES), F32)],
        [ids, tokens, partial, swap(partial), post_gain, branch_gate, notes],
    )
    near = []
    for k in range(1, planes):
        near.append(exchange(payload, k * plane))
    wide = [dense_gate_w, dense_up_w, expert_gate_w[0], expert_up_w[0]]
    gate_w, up_w, expert_gate, expert_up = call(
        fetch_kernel,
        [(value.shape, BF16) for value in wide],
        [payload, *wide],
        hbm=range(1, 5),
        scratch=[pltpu.SemaphoreType.DMA((4,))],
    )
    column = jnp.concatenate([payload] + near, axis=0)
    owns = [column] + [None] * (plane - 1)
    for j in reversed(range(1, plane)):
        owns[j] = exchange(column, j)
    combine, down_own, expert_own, down_sent = call(
        functools.partial(load_kernel, seq=seq, capacity=capacity, top_k=top_k),
        [
            ((plane, planes * pair_rows, planes * capacity), BF16),
            ((ff_local, half), BF16),
            ((expert_local, half), BF16),
            ((ff_local + expert_local, half), BF16),
        ],
        [ids, column, dense_down_w, expert_down_w[0]],
        hbm=range(2, 4),
        scratch=[pltpu.SemaphoreType.DMA((4,))],
    )
    down_got = swap(down_sent)
    others = []
    for j in range(plane):
        others.append(swap(owns[j]))
    arrived = [None] * plane
    order = [0] + list(reversed(range(1, plane)))
    for members in (order[: plane // 2], order[plane // 2 :]):
        size = len(members)
        rows, routes = size * planes * seq, size * planes * capacity
        extra = 8 * ((2 * size + 7) // 8)
        hidden, slot_weight = call(
            functools.partial(hidden_kernel, seq=seq, capacity=capacity, top_k=top_k),
            [((rows + routes + extra, widest), BF16), ((routes, LANES), F32)],
            [
                ids, *[owns[j] for j in members], *[others[j] for j in members],
                gate_w, up_w, expert_gate, expert_up,
            ],
            scratch=[
                pltpu.VMEM((rows, half), BF16), pltpu.VMEM((rows, half), BF16),
                pltpu.VMEM((rows, LANES), F32),
            ],
        )
        hidden_other = swap(hidden)
        sums = call(
            functools.partial(down_kernel, count=rows),
            [((planes * (seq + capacity) + 8, half), BF16)] * size,
            [hidden, hidden_other, down_own, expert_own, down_got, slot_weight],
        )
        for j, value in zip(members, sums):
            arrived[j] = exchange(value, j) if j else value
    lasts = call(
        functools.partial(plane_kernel, planes=planes, seq=seq, capacity=capacity),
        [((seq + pair_rows, half), BF16)] * planes,
        [*arrived, combine],
    )
    final = [lasts[0]] + [exchange(lasts[k], k * plane) for k in range(1, planes)]
    (mixed_out,) = call(
        functools.partial(
            final_kernel, ff_total=ff_total, route_base=capacity * plane, top_k=top_k
        ),
        [((seq, half), BF16)],
        [z_peers, *final, resid, branch, notes],
    )
    return (mixed_out, fresh_key, fresh_value, current)


def solution(mesh):
    placed = (
        P("ep", None), P(), P(None, "tp"), P(), P(), P(), P(), P(), P(),
        P("ep", "tp", None, None), P("ep", "tp", None, None), P("ep", "tp", None), P("ep"),
        P("tp", None), P(), P(),
        P(None, ("ep", "tp")), P(None, ("ep", "tp")), P(("ep", "tp"), None),
        P("ep", None), P("ep", None),
        P("ep", None, "tp"), P("ep", None, "tp"), P("ep", "tp", None),
    )
    return jax.shard_map(
        body,
        mesh=mesh,
        in_specs=placed,
        out_specs=(P("ep", "tp"), P("ep", "tp", None), P("ep", "tp", None), P("ep", "tp")),
        check_vma=False,
    )
```

```python
import functools

import jax
import jax.numpy as jnp
from jax import lax
from jax.experimental import pallas as pl
from jax.experimental.pallas import tpu as pltpu
from jax.sharding import PartitionSpec as P


GROUPS = 4
LANES = 128
BLOCK_KEY = 1024.0

norm_eps = 1e-06


def rms_scale(values, gain_vec):
    mean_square = jnp.mean(values * values, axis=-1, keepdims=True)
    return values * lax.rsqrt(mean_square + norm_eps) * gain_vec


def split_two(values):
    high = values.astype(jnp.bfloat16)
    low = (values - high.astype(jnp.float32)).astype(jnp.bfloat16)
    return high, low


def route_slots(expert_choice, ep_count, capacity):
    route_ids = expert_choice.reshape(-1)
    member = (route_ids[:, None] == jnp.arange(ep_count)[None, :]).astype(jnp.float32)
    count = route_ids.shape[0]
    earlier = (
        lax.broadcasted_iota(jnp.int32, (count, count), 0)
        > lax.broadcasted_iota(jnp.int32, (count, count), 1)
    ).astype(jnp.float32)
    before = jnp.dot(earlier, member, preferred_element_type=jnp.float32)
    rank = jnp.sum(before * member, axis=1)
    slot = route_ids.astype(jnp.float32) * capacity + rank
    return slot.reshape(expert_choice.shape)


F32, BF16 = jnp.float32, jnp.bfloat16
VMEM = pl.BlockSpec(memory_space=pltpu.VMEM)
SMEM = pl.BlockSpec(memory_space=pltpu.SMEM)


def call(kernel, outs, operands, hbm=(), scratch=(), limit=20, kept=True):
    specs = []
    held = []
    for index, op in enumerate(operands):
        if index in hbm:
            specs.append(pl.BlockSpec(memory_space=pltpu.HBM))
            held.append(pltpu.with_memory_space_constraint(op, pltpu.HBM))
        elif op.dtype == jnp.int32 and op.ndim == 1:
            specs.append(SMEM)
            held.append(op)
        else:
            specs.append(VMEM)
            held.append(pltpu.with_memory_space_constraint(op, pltpu.VMEM))
    return pl.pallas_call(
        kernel,
        in_specs=specs,
        out_specs=[VMEM] * len(outs),
        out_shape=[(pltpu.VMEM if kept else jax.ShapeDtypeStruct)(shape, dtype) for shape, dtype in outs],
        scratch_shapes=list(scratch),
        compiler_params=pltpu.CompilerParams(vmem_limit_bytes=limit * 1024 * 1024),
    )(*held)


def axis_iota(shape, axis):
    return lax.broadcasted_iota(jnp.int32, shape, axis).astype(F32)


def block_of(index, size):
    return jnp.floor((index + 0.5) * (1.0 / size))


def dot(left, right):
    return jnp.dot(left, right, preferred_element_type=F32)


def high_low(values):
    high = values.astype(BF16).astype(F32)
    return high, values - high


def to_row(column):
    rows = column.shape[0]
    wide = jnp.broadcast_to(column, (rows, LANES))
    if rows < LANES:
        wide = jnp.concatenate([wide, jnp.zeros((LANES - rows, LANES), F32)], axis=0)
    return jnp.transpose(wide)[0:1]


def silu(values):
    return values / (1.0 + jnp.exp(-values))


def post_kernel(ids, tokens, part_a, part_b, gain, branch_gate, notes, payload, resid, branch):
    half = resid.shape[1]
    first = ids[0] == 0
    total = tokens[...].astype(F32) + (part_a[...].astype(F32) + part_b[...].astype(F32))
    total = total.astype(BF16).astype(F32)
    mean_square = jnp.mean(total * total, axis=-1, keepdims=True)
    post = (total * lax.rsqrt(mean_square + norm_eps) * gain[...].astype(F32)[None]).astype(BF16)
    gate = jnp.sum(post.astype(F32) * branch_gate[...].astype(F32)[None], axis=-1, keepdims=True)
    branch[...] = jnp.broadcast_to(1.0 / (1.0 + jnp.exp(-gate)), branch.shape)
    payload[:, :half] = jnp.where(first, post[:, :half], post[:, half:])
    payload[:, half:] = notes[...]
    resid[...] = jnp.where(first, total[:, :half], total[:, half:]).astype(BF16)


def fetch_kernel(
    ids, anchor, gate_in, up_in, expert_gate_in, expert_up_in, down_in, expert_in,
    down_sent, gate_w, up_w, expert_gate, expert_up, sems,
):
    hidden, half = down_in.shape[0], down_sent.shape[1]
    other = expert_in.shape[0]
    theirs = pl.ds(pl.multiple_of((1 - ids[0]) * half, half), half)
    pairs = [
        (down_in.at[:, theirs], down_sent.at[pl.ds(0, hidden)]),
        (expert_in.at[:, theirs], down_sent.at[pl.ds(hidden, other)]),
        (gate_in, gate_w), (up_in, up_w), (expert_gate_in, expert_gate),
        (expert_up_in, expert_up),
    ]
    copies = [pltpu.make_async_copy(a, b, sems.at[i]) for i, (a, b) in enumerate(pairs)]
    for copy in copies:
        copy.start()
    for copy in copies:
        copy.wait()


def load_kernel(ids, column, down_in, expert_in, down_own, expert_own, sems):
    half = down_own.shape[1]
    mine = pl.ds(pl.multiple_of(ids[0] * half, half), half)
    pairs = [(down_in.at[:, mine], down_own), (expert_in.at[:, mine], expert_own)]
    copies = [pltpu.make_async_copy(a, b, sems.at[i]) for i, (a, b) in enumerate(pairs)]
    for copy in copies:
        copy.start()
    for copy in copies:
        copy.wait()


def table_kernel(ids, column, combine, *, seq, capacity, top_k):
    plane = combine.shape[0]
    planes = combine.shape[2] // capacity
    pair_rows = combine.shape[1] // planes
    tokens = planes * seq
    info = column[:, column.shape[1] - LANES :].astype(F32)
    near_key = block_of(axis_iota((tokens, 1), 0), seq) * BLOCK_KEY
    lane = axis_iota((1, planes * capacity), 1)
    lane_block = block_of(lane, capacity)
    lane_key = lane_block * BLOCK_KEY + (lane - lane_block * capacity)
    pair = axis_iota((planes * pair_rows, 1), 0)
    pair_block = block_of(pair, pair_rows)
    pair_offset = pair - pair_block * pair_rows
    pair_id = jnp.where(pair_offset < seq // 2, pair_block * (seq // 2) + pair_offset, -1.0)
    joined = (block_of(axis_iota((1, tokens), 1), 2) == pair_id).astype(BF16)
    for j in range(plane):
        match = jnp.zeros((tokens, planes * capacity), F32)
        for k in range(top_k):
            match = match + (
                info[:, k : k + 1] + near_key == lane_key + ids[2 + j].astype(F32)
            ).astype(F32)
        combine[j] = dot(joined, match.astype(BF16)).astype(BF16)


def hidden_kernel(ids, *refs, seq, capacity, top_k):
    plane = (len(refs) - 8) // 2
    owns, others = refs[:plane], refs[plane : 2 * plane]
    gate_w, up_w, expert_gate, expert_up, out, slot_weight, tokens, notes = refs[2 * plane :]
    count = tokens.shape[0]
    half = tokens.shape[1] // 2
    slots = slot_weight.shape[0]
    group = count // plane
    own_part = pl.ds(pl.multiple_of(ids[0] * half, half), half)
    other_part = pl.ds(pl.multiple_of((1 - ids[0]) * half, half), half)
    for j in range(plane):
        rows = pl.ds(j * group, group)
        tokens[rows, own_part] = owns[j][:, :half]
        tokens[rows, other_part] = others[j][:, :half]
        notes[rows, :] = owns[j][:, half:].astype(F32)
    all_rows = tokens[...]
    hidden = silu(dot(all_rows, gate_w[...])) * dot(all_rows, up_w[...])
    out[0:count, 0 : gate_w.shape[1]] = hidden.astype(BF16)
    squares = jnp.sum(hidden * hidden, axis=1, keepdims=True)
    extra = out.shape[0] - count - slots
    tile_row = lax.broadcasted_iota(jnp.int32, (extra, LANES), 0)
    tile = jnp.zeros((extra, LANES), F32)
    for j in range(plane):
        high, low = high_low(to_row(squares[j * group : (j + 1) * group]))
        tile = jnp.where(tile_row == 2 * j, high, jnp.where(tile_row == 2 * j + 1, low, tile))
    out[count + slots :, :] = jnp.zeros((extra, out.shape[1]), BF16)
    out[count + slots :, 0:LANES] = tile.astype(BF16)

    turned = jnp.transpose(notes[...])
    token = axis_iota((1, count), 1)
    token_key = block_of(token, seq) * BLOCK_KEY
    slot = axis_iota((slots, 1), 0)
    slot_block = block_of(slot, capacity)
    slot_key = slot_block * BLOCK_KEY + (slot - slot_block * capacity) + ids[1].astype(F32)
    pick = jnp.zeros((slots, count), F32)
    weight = jnp.zeros((slots, count), F32)
    for k in range(top_k):
        hit = (turned[k : k + 1] + token_key == slot_key).astype(F32)
        value = turned[top_k + k : top_k + k + 1] + turned[2 * top_k + k : 2 * top_k + k + 1]
        pick = pick + hit
        weight = weight + hit * value
    slot_weight[...] = jnp.broadcast_to(
        jnp.sum(weight, axis=1, keepdims=True), slot_weight.shape
    )
    pick = pick.astype(BF16)
    picked = dot(pick, all_rows).astype(BF16)
    active = silu(dot(picked, expert_gate[...])) * dot(picked, expert_up[...])
    out[count : count + slots, 0 : expert_gate.shape[1]] = active.astype(BF16)


def down_kernel(own, other, down_own, expert_own, down_got, slot_weight, *outs, count):
    plane = len(outs)
    half = outs[0].shape[1]
    slots = slot_weight.shape[0]
    hidden, routed_hidden = down_own.shape[0], expert_own.shape[0]
    dense = dot(own[0:count, 0:hidden], down_own[...]) + dot(
        other[0:count, 0:hidden], down_got[0:hidden, :]
    )
    routed_rows = slice(count, count + slots)
    routed = dot(own[routed_rows, 0:routed_hidden], expert_own[...]) + dot(
        other[routed_rows, 0:routed_hidden], down_got[hidden:, :]
    )
    routed = routed * slot_weight[:, 0:1]
    squares = own[count + slots :, 0:LANES].astype(F32) + other[count + slots :, 0:LANES].astype(F32)
    group, part = count // plane, slots // plane
    tile_row = lax.broadcasted_iota(jnp.int32, (8, LANES), 0)
    for j in range(plane):
        outs[j][0:group, :] = dense[j * group : (j + 1) * group].astype(BF16)
        outs[j][group : group + part, :] = routed[j * part : (j + 1) * part].astype(BF16)
        high, low = high_low(squares[2 * j : 2 * j + 1] + squares[2 * j + 1 : 2 * j + 2])
        outs[j][group + part :, :] = jnp.zeros((8, half), BF16)
        outs[j][group + part :, 0:LANES] = jnp.where(
            tile_row == 0, high, jnp.where(tile_row == 1, low, 0.0)
        ).astype(BF16)


def plane_kernel(*refs, planes, seq, capacity):
    plane = len(refs) - planes - 1
    parts, combine, outs = refs[:plane], refs[plane], refs[plane + 1 :]
    group, part = planes * seq, planes * capacity
    dense = parts[0][0:group, :].astype(F32)
    routed = dot(combine[0], parts[0][group : group + part, :])
    notes = parts[0][group + part :, 0:LANES].astype(F32)
    for j in range(1, plane):
        dense = dense + parts[j][0:group, :].astype(F32)
        routed = routed + dot(combine[j], parts[j][group : group + part, :])
        notes = notes + parts[j][group + part :, 0:LANES].astype(F32)
    high, low = high_low(notes[0:1] + notes[1:2])
    pair_rows = combine.shape[1] // planes
    tile_row = lax.broadcasted_iota(jnp.int32, (pair_rows, LANES), 0)
    for k in range(planes):
        outs[k][0:seq, :] = dense[k * seq : (k + 1) * seq].astype(BF16)
        tail = routed[k * pair_rows : (k + 1) * pair_rows]
        first = jnp.where(
            tile_row == seq // 2,
            high,
            jnp.where(tile_row == seq // 2 + 1, low, tail[:, 0:LANES]),
        )
        outs[k][seq:, 0:LANES] = first.astype(BF16)
        outs[k][seq:, LANES:] = tail[:, LANES:].astype(BF16)


def final_kernel(*refs, ff_total, route_base, top_k):
    planes = len(refs) - 5
    ids, parts = refs[0], refs[1 : 1 + planes]
    resid, branch, notes, out = refs[1 + planes :]
    seq = resid.shape[0]
    half_seq = seq // 2
    pair_rows = parts[0].shape[0] - seq
    group = block_of(notes[:, 0:1].astype(F32), route_base)
    token_pair = block_of(axis_iota((seq, 1), 0), 2)
    lane = axis_iota((1, pair_rows), 1)
    dense = jnp.zeros(out.shape, F32)
    routed = jnp.zeros(out.shape, F32)
    squares = jnp.zeros((seq, LANES), F32)
    for k in range(planes):
        dense = dense + parts[k][0:seq, :].astype(F32)
        tail = parts[k][seq:, :]
        place = jnp.where(
            (token_pair == lane) & (group == ids[k].astype(F32)), 1.0, 0.0
        ).astype(BF16)
        routed = routed + dot(place, tail)
        values = tail[:, 0:LANES].astype(F32)
        row = values[half_seq : half_seq + 1] + values[half_seq + 1 : half_seq + 2]
        turned = jnp.transpose(jnp.broadcast_to(row, (LANES, LANES)))
        squares = squares + turned[k * seq : (k + 1) * seq]
    scale = branch[:, 0:1] * lax.rsqrt(squares[:, 0:1] * (1.0 / ff_total) + norm_eps)
    out[...] = (resid[...].astype(F32) + routed + scale * dense).astype(BF16)


def attend_kernel(
    ids, lens_in, tokens_in, norm_in, query_in, key_in, bias_in,
    query_w, key_w, value_w, forget_w, cache_key, cache_value, cache_gate, out_w,
    partial, fresh_key, fresh_value, fresh_gate,
    q_w, k_w, v_w, f_w, keys, values, gates, o_w, q_rows, k_rows, v_rows, f_cols, g_cols, mixed,
    tokens, norm_gain, query_gain, key_gain, forget_bias, lens, sems,
    *, heads, chunks,
):
    seq = tokens.shape[0]
    head = cache_key.shape[1]
    span = cache_key.shape[2]
    step = seq // chunks
    plain = [
        (tokens_in, tokens), (norm_in, norm_gain), (query_in, query_gain), (key_in, key_gain),
        (bias_in, forget_bias), (lens_in, lens), (key_w, k_w), (value_w, v_w), (forget_w, f_w), (query_w, q_w),
    ]
    small = [pltpu.make_async_copy(a, b, sems.at[i]) for i, (a, b) in enumerate(plain)]
    base = len(small)
    parts = []
    for c in range(chunks):
        rows = pl.ds(c * step, step)
        for a, b in ((cache_key, keys), (cache_gate, gates), (cache_value, values)):
            parts.append(pltpu.make_async_copy(a.at[rows], b.at[rows], sems.at[base + len(parts)]))
    last = pltpu.make_async_copy(out_w, o_w, sems.at[base + len(parts)])
    for copy in small + parts + [last]:
        copy.start()
    for copy in small[:6]:
        copy.wait()
    small = small[6:]
    first = ids[0] == 0
    resid = tokens[...].astype(F32)
    mean_square = jnp.mean(resid * resid, axis=-1, keepdims=True)
    normed = (resid * lax.rsqrt(mean_square + norm_eps) * norm_gain[...].astype(F32)[None]).astype(BF16)
    small[0].wait()
    key = dot(normed, k_w[...])
    key = jnp.where(first, key[:, :head], key[:, head:])
    key = rms_scale(key, key_gain[...].astype(F32)[None]).astype(BF16)
    fresh_key[...] = key
    k_rows[...] = key.astype(F32)
    small[1].wait()
    value = dot(normed, v_w[...])
    value = jnp.where(first, value[:, :head], value[:, head:]).astype(BF16)
    fresh_value[...] = value
    v_rows[...] = value.astype(F32)
    small[2].wait()
    forget = lax.dot_general(
        normed, f_w[...], (((1,), (1,)), ((), ())), preferred_element_type=F32
    )
    forget = forget + forget_bias[...][None]
    forget = jnp.minimum(forget, 0.0) - jnp.log1p(jnp.exp(-jnp.abs(forget)))
    forget = jnp.where(first, forget[:, :heads], forget[:, heads:])
    wide = jnp.concatenate([forget, jnp.zeros((seq, LANES - heads), F32)], axis=1)
    wide = jnp.concatenate([wide, jnp.zeros((LANES - seq, LANES), F32)], axis=0)
    f_cols[...] = jnp.transpose(wide)[0:heads]
    small[3].wait()
    queries = dot(normed, q_w[...])
    scale = head ** (-0.5)
    for h in range(heads):
        part = queries[:, h * head : (h + 1) * head]
        part = rms_scale(part, query_gain[...].astype(F32)[None]).astype(BF16)
        q_rows[:, h, :] = part.astype(F32) * scale
    g_cols[...] = jnp.zeros(g_cols.shape, F32)
    lane = lax.broadcasted_iota(jnp.int32, (heads, span), 1)
    lane_small = lax.broadcasted_iota(jnp.int32, (heads, LANES), 1)

    def several(span_of):
        lengths = [lens[s] for s in span_of]
        place = [length - 1 for length in lengths]
        block = [pl.multiple_of((at // LANES) * LANES, LANES) for at in place]
        near = [gates[s, :, pl.ds(at, LANES)] for s, at in zip(span_of, block)]
        previous = [
            jnp.sum(jnp.where(lane_small == at - start, value, 0.0), axis=1, keepdims=True)
            for at, start, value in zip(place, block, near)
        ]
        current = [f_cols[:, s : s + 1] + value for s, value in zip(span_of, previous)]
        for s, value in zip(span_of, current):
            g_cols[:, s : s + 1] = value
        query = [q_rows[s] for s in span_of]
        scores = [dot(value.astype(BF16), keys[s]) for s, value in zip(span_of, query)]
        own = [
            jnp.sum(value * k_rows[s : s + 1], axis=1, keepdims=True)
            for s, value in zip(span_of, query)
        ]
        logits = [
            jnp.where(lane < length, score + (now - gates[s]), -1e30)
            for s, length, score, now in zip(span_of, lengths, scores, current)
        ]
        top = [
            jnp.maximum(jnp.max(value, axis=1, keepdims=True), mine)
            for value, mine in zip(logits, own)
        ]
        weight = [jnp.exp(value - peak) for value, peak in zip(logits, top)]
        own_weight = [jnp.exp(mine - peak) for mine, peak in zip(own, top)]
        inverse = [
            1.0 / (jnp.sum(value, axis=1, keepdims=True) + mine)
            for value, mine in zip(weight, own_weight)
        ]
        probs = [(value * factor).astype(BF16) for value, factor in zip(weight, inverse)]
        out = [
            lax.dot_general(
                value, values[s], (((1,), (1,)), ((), ())), preferred_element_type=F32
            )
            for s, value in zip(span_of, probs)
        ]
        for s, value, mine, factor in zip(span_of, out, own_weight, inverse):
            own_prob = (mine * factor).astype(BF16).astype(F32)
            mixed[s] = value + own_prob * v_rows[s : s + 1]

    for c in range(chunks):
        for copy in parts[3 * c : 3 * c + 3]:
            copy.wait()
        for start in range(c * step, (c + 1) * step, 12):
            several(range(start, min(start + 12, (c + 1) * step)))
    turned = jnp.concatenate([g_cols[...], jnp.zeros((LANES - heads, LANES), F32)], axis=0)
    fresh_gate[...] = jnp.transpose(turned)[0:seq, 0:heads]
    last.wait()
    total = jnp.zeros(partial.shape, F32)
    for h in range(heads):
        total = total + dot(mixed[:, h, :].astype(BF16), o_w[h * head : (h + 1) * head, :])
    partial[...] = total.astype(BF16)


def attend(
    ids, tokens, norm_gain, query_w, key_w, value_w, forget_w, forget_bias,
    query_gain, key_gain, cache_key, cache_value, cache_gate, cache_len, out_w,
):
    seq, width = tokens.shape
    heads = cache_gate.shape[1]
    head, span = cache_key.shape[2:]
    chunks = 2 if seq % 2 == 0 else 1
    scratch = [
        pltpu.VMEM(query_w.shape, BF16), pltpu.VMEM(key_w.shape, BF16),
        pltpu.VMEM(value_w.shape, BF16), pltpu.VMEM(forget_w.shape[::-1], BF16),
        pltpu.VMEM((seq, head, span), BF16), pltpu.VMEM((seq, head, span), BF16),
        pltpu.VMEM((seq, heads, span), F32), pltpu.VMEM(out_w.shape, BF16),
        pltpu.VMEM((seq, heads, head), F32), pltpu.VMEM((seq, head), F32),
        pltpu.VMEM((seq, head), F32), pltpu.VMEM((heads, LANES), F32),
        pltpu.VMEM((heads, LANES), F32), pltpu.VMEM((seq, heads, head), F32),
        pltpu.VMEM(tokens.shape, BF16), pltpu.VMEM(norm_gain.shape, BF16),
        pltpu.VMEM(query_gain.shape, BF16), pltpu.VMEM(key_gain.shape, BF16),
        pltpu.VMEM(forget_bias.shape, F32), pltpu.SMEM(cache_len.shape, jnp.int32),
        pltpu.SemaphoreType.DMA((11 + 3 * chunks,)),
    ]
    partial, fresh_key, fresh_value, current = call(
        functools.partial(attend_kernel, heads=heads, chunks=chunks),
        [((seq, width), BF16), ((seq, head), BF16), ((seq, head), BF16), ((seq, heads), F32)],
        [
            ids, cache_len, tokens, norm_gain, query_gain, key_gain, forget_bias, query_w, key_w, value_w, forget_w.T,
            cache_key[:, 0], cache_value[:, 0], cache_gate, out_w,
        ],
        hbm=range(1, 15),
        scratch=scratch,
        limit=32,
    )
    return partial, fresh_key[:, None], fresh_value[:, None], current


def body(
    tokens, norm_gain, query_w, key_w, value_w, forget_w, forget_bias, query_gain, key_gain,
    cache_key, cache_value, cache_gate, cache_len, out_w, post_gain, branch_gate,
    dense_gate_w, dense_up_w, dense_down_w, expert_choice, route_weight,
    expert_gate_w, expert_up_w, expert_down_w,
):
    seq, width = tokens.shape
    tp_count = lax.axis_size("tp")
    ep_count = lax.axis_size("ep")
    tp_rank = lax.axis_index("tp")
    ep_rank = lax.axis_index("ep")
    half = width // tp_count
    planes = GROUPS
    plane = ep_count // planes
    capacity = 2 * ((seq + 2 * plane - 1) // (2 * plane))
    top_k = expert_choice.shape[1]
    ff_local = dense_gate_w.shape[1]
    expert_local = expert_gate_w.shape[2]
    widest = max(ff_local, expert_local)
    ff_total = ff_local * ep_count * tp_count
    pair_rows = 8 * ((seq // 2 + 2 + 7) // 8)
    z_rank = ep_rank // plane
    p_rank = ep_rank % plane

    def swap(values):
        return lax.ppermute(values, "tp", [(i, 1 - i) for i in range(tp_count)])

    def exchange(values, mask):
        return lax.ppermute(values, "ep", [(i, i ^ mask) for i in range(ep_count)])

    slot_ids = route_slots(expert_choice, ep_count, capacity)
    weight_high, weight_low = split_two(route_weight)
    notes = jnp.concatenate([slot_ids.astype(BF16), weight_high, weight_low], axis=1)
    notes = jnp.pad(notes, ((0, 0), (0, LANES - notes.shape[1])))
    peers = jnp.bitwise_xor(jnp.arange(plane, dtype=jnp.int32), p_rank) + z_rank * plane
    ids = jnp.concatenate([jnp.stack([tp_rank, ep_rank * capacity]), peers * capacity])
    ids = ids.astype(jnp.int32)
    z_peers = jnp.bitwise_xor(jnp.arange(planes, dtype=jnp.int32), z_rank)

    partial, fresh_key, fresh_value, current = attend(
        ids, tokens, norm_gain, query_w, key_w, value_w, forget_w, forget_bias,
        query_gain, key_gain, cache_key, cache_value, cache_gate, cache_len, out_w,
    )
    payload, resid, branch = call(
        post_kernel,
        [((seq, half + LANES), BF16), ((seq, half), BF16), ((seq, LANES), F32)],
        [ids, tokens, partial, swap(partial), post_gain, branch_gate, notes],
    )
    near = [None] * planes
    for k in reversed(range(1, planes)):
        near[k] = exchange(payload, k * plane)
    wide = [dense_gate_w, dense_up_w, expert_gate_w[0], expert_up_w[0]]
    down_sent, gate_w, up_w, expert_gate, expert_up = call(
        fetch_kernel,
        [((ff_local + expert_local, half), BF16)] + [(value.shape, BF16) for value in wide],
        [ids, payload, *wide, dense_down_w, expert_down_w[0]],
        hbm=range(2, 8),
        scratch=[pltpu.SemaphoreType.DMA((6,))],
    )
    column = jnp.concatenate([payload] + near[1:], axis=0)
    owns = [column] + [None] * (plane - 1)
    for j in reversed(range(1, plane)):
        owns[j] = exchange(column, j)
    down_own, expert_own = call(
        load_kernel,
        [((ff_local, half), BF16), ((expert_local, half), BF16)],
        [ids, column, dense_down_w, expert_down_w[0]],
        hbm=range(2, 4),
        scratch=[pltpu.SemaphoreType.DMA((2,))],
    )
    (combine,) = call(
        functools.partial(table_kernel, seq=seq, capacity=capacity, top_k=top_k),
        [((plane, planes * pair_rows, planes * capacity), BF16)],
        [ids, column],
    )
    down_got = swap(down_sent)
    others = []
    for j in range(plane):
        others.append(swap(owns[j]))
    arrived = [None] * plane
    order = list(reversed(range(1, plane)))
    early, late = order[: plane // 2 - 1], order[plane // 2 - 1 :]
    for members in ([0] + early, late):
        size = len(members)
        rows, routes = size * planes * seq, size * planes * capacity
        extra = 8 * ((2 * size + 7) // 8)
        hidden, slot_weight = call(
            functools.partial(hidden_kernel, seq=seq, capacity=capacity, top_k=top_k),
            [((rows + routes + extra, widest), BF16), ((routes, LANES), F32)],
            [
                ids, *[owns[j] for j in members], *[others[j] for j in members],
                gate_w, up_w, expert_gate, expert_up,
            ],
            scratch=[
                pltpu.VMEM((rows, width), BF16), pltpu.VMEM((rows, LANES), F32),
            ],
        )
        hidden_other = swap(hidden)
        sums = call(
            functools.partial(down_kernel, count=rows),
            [((planes * (seq + capacity) + 8, half), BF16)] * size,
            [hidden, hidden_other, down_own, expert_own, down_got, slot_weight],
        )
        for j, value in zip(members, sums):
            arrived[j] = exchange(value, j) if j else value
    lasts = call(
        functools.partial(plane_kernel, planes=planes, seq=seq, capacity=capacity),
        [((seq + pair_rows, half), BF16)] * planes,
        [*arrived, combine],
    )
    final = [lasts[0]] + [None] * (planes - 1)
    for k in reversed(range(1, planes)):
        final[k] = exchange(lasts[k], k * plane)
    (mixed_out,) = call(
        functools.partial(
            final_kernel, ff_total=ff_total, route_base=capacity * plane, top_k=top_k
        ),
        [((seq, half), BF16)],
        [z_peers, *final, resid, branch, notes],
        kept=True,
    )
    return (mixed_out, fresh_key, fresh_value, current)


def solution(mesh):
    placed = (
        P("ep", None), P(), P(None, "tp"), P(), P(), P(), P(), P(), P(),
        P("ep", "tp", None, None), P("ep", "tp", None, None), P("ep", "tp", None), P("ep"),
        P("tp", None), P(), P(),
        P(None, ("ep", "tp")), P(None, ("ep", "tp")), P(("ep", "tp"), None),
        P("ep", None), P("ep", None),
        P("ep", None, "tp"), P("ep", None, "tp"), P("ep", "tp", None),
    )
    return jax.shard_map(
        body,
        mesh=mesh,
        in_specs=placed,
        out_specs=(P("ep", "tp"), P("ep", "tp", None), P("ep", "tp", None), P("ep", "tp")),
        check_vma=False,
    )
```

```python
import functools

import jax
import jax.numpy as jnp
from jax import lax
from jax.experimental import pallas as pl
from jax.experimental.pallas import tpu as pltpu
from jax.sharding import PartitionSpec as P


GROUPS = 4
LANES = 128
BLOCK_KEY = 1024.0

norm_eps = 1e-06


def rms_scale(values, gain_vec):
    mean_square = jnp.mean(values * values, axis=-1, keepdims=True)
    return values * lax.rsqrt(mean_square + norm_eps) * gain_vec


def split_two(values):
    high = values.astype(jnp.bfloat16)
    low = (values - high.astype(jnp.float32)).astype(jnp.bfloat16)
    return high, low


def route_slots(expert_choice, ep_count, capacity):
    route_ids = expert_choice.reshape(-1)
    member = (route_ids[:, None] == jnp.arange(ep_count)[None, :]).astype(jnp.float32)
    count = route_ids.shape[0]
    earlier = (
        lax.broadcasted_iota(jnp.int32, (count, count), 0)
        > lax.broadcasted_iota(jnp.int32, (count, count), 1)
    ).astype(jnp.float32)
    before = jnp.dot(earlier, member, preferred_element_type=jnp.float32)
    rank = jnp.sum(before * member, axis=1)
    slot = route_ids.astype(jnp.float32) * capacity + rank
    return slot.reshape(expert_choice.shape)


F32, BF16 = jnp.float32, jnp.bfloat16
VMEM = pl.BlockSpec(memory_space=pltpu.VMEM)
SMEM = pl.BlockSpec(memory_space=pltpu.SMEM)


def call(kernel, outs, operands, hbm=(), scratch=(), limit=20, kept=True):
    specs = []
    held = []
    for index, op in enumerate(operands):
        if index in hbm:
            specs.append(pl.BlockSpec(memory_space=pltpu.HBM))
            held.append(pltpu.with_memory_space_constraint(op, pltpu.HBM))
        elif op.dtype == jnp.int32 and op.ndim == 1:
            specs.append(SMEM)
            held.append(op)
        else:
            specs.append(VMEM)
            held.append(pltpu.with_memory_space_constraint(op, pltpu.VMEM))
    return pl.pallas_call(
        kernel,
        in_specs=specs,
        out_specs=[VMEM] * len(outs),
        out_shape=[(pltpu.VMEM if kept else jax.ShapeDtypeStruct)(shape, dtype) for shape, dtype in outs],
        scratch_shapes=list(scratch),
        compiler_params=pltpu.CompilerParams(vmem_limit_bytes=limit * 1024 * 1024),
    )(*held)


def axis_iota(shape, axis):
    return lax.broadcasted_iota(jnp.int32, shape, axis).astype(F32)


def block_of(index, size):
    return jnp.floor((index + 0.5) * (1.0 / size))


def dot(left, right):
    return jnp.dot(left, right, preferred_element_type=F32)


def high_low(values):
    high = values.astype(BF16).astype(F32)
    return high, values - high


def to_row(column):
    rows = column.shape[0]
    wide = jnp.broadcast_to(column, (rows, LANES))
    if rows < LANES:
        wide = jnp.concatenate([wide, jnp.zeros((LANES - rows, LANES), F32)], axis=0)
    return jnp.transpose(wide)[0:1]


def silu(values):
    return values / (1.0 + jnp.exp(-values))


def post_kernel(ids, tokens, part_a, part_b, gain, branch_gate, notes, payload, resid, branch):
    half = resid.shape[1]
    first = ids[0] == 0
    total = tokens[...].astype(F32) + (part_a[...].astype(F32) + part_b[...].astype(F32))
    total = total.astype(BF16).astype(F32)
    mean_square = jnp.mean(total * total, axis=-1, keepdims=True)
    post = (total * lax.rsqrt(mean_square + norm_eps) * gain[...].astype(F32)[None]).astype(BF16)
    gate = jnp.sum(post.astype(F32) * branch_gate[...].astype(F32)[None], axis=-1, keepdims=True)
    branch[...] = jnp.broadcast_to(1.0 / (1.0 + jnp.exp(-gate)), branch.shape)
    payload[:, :half] = jnp.where(first, post[:, :half], post[:, half:])
    payload[:, half:] = notes[...]
    resid[...] = jnp.where(first, total[:, :half], total[:, half:]).astype(BF16)


def fetch_kernel(
    ids, anchor, gate_in, up_in, expert_gate_in, expert_up_in, down_in, expert_in,
    down_sent, gate_w, up_w, expert_gate, expert_up, sems,
):
    hidden, half = down_in.shape[0], down_sent.shape[1]
    other = expert_in.shape[0]
    theirs = pl.ds(pl.multiple_of((1 - ids[0]) * half, half), half)
    pairs = [
        (down_in.at[:, theirs], down_sent.at[pl.ds(0, hidden)]),
        (expert_in.at[:, theirs], down_sent.at[pl.ds(hidden, other)]),
        (gate_in, gate_w), (up_in, up_w), (expert_gate_in, expert_gate),
        (expert_up_in, expert_up),
    ]
    copies = [pltpu.make_async_copy(a, b, sems.at[i]) for i, (a, b) in enumerate(pairs)]
    for copy in copies:
        copy.start()
    for copy in copies:
        copy.wait()


def load_kernel(ids, column, down_in, expert_in, down_own, expert_own, sems):
    half = down_own.shape[1]
    mine = pl.ds(pl.multiple_of(ids[0] * half, half), half)
    pairs = [(down_in.at[:, mine], down_own), (expert_in.at[:, mine], expert_own)]
    copies = [pltpu.make_async_copy(a, b, sems.at[i]) for i, (a, b) in enumerate(pairs)]
    for copy in copies:
        copy.start()
    for copy in copies:
        copy.wait()


def table_kernel(ids, column, combine, *, seq, capacity, top_k):
    plane = combine.shape[0]
    planes = combine.shape[2] // capacity
    pair_rows = combine.shape[1] // planes
    tokens = planes * seq
    info = column[:, column.shape[1] - LANES :].astype(F32)
    near_key = block_of(axis_iota((tokens, 1), 0), seq) * BLOCK_KEY
    lane = axis_iota((1, planes * capacity), 1)
    lane_block = block_of(lane, capacity)
    lane_key = lane_block * BLOCK_KEY + (lane - lane_block * capacity)
    pair = axis_iota((planes * pair_rows, 1), 0)
    pair_block = block_of(pair, pair_rows)
    pair_offset = pair - pair_block * pair_rows
    pair_id = jnp.where(pair_offset < seq // 2, pair_block * (seq // 2) + pair_offset, -1.0)
    joined = (block_of(axis_iota((1, tokens), 1), 2) == pair_id).astype(BF16)
    for j in range(plane):
        match = jnp.zeros((tokens, planes * capacity), F32)
        for k in range(top_k):
            match = match + (
                info[:, k : k + 1] + near_key == lane_key + ids[2 + j].astype(F32)
            ).astype(F32)
        combine[j] = dot(joined, match.astype(BF16)).astype(BF16)


def hidden_kernel(ids, *refs, seq, capacity, top_k):
    plane = (len(refs) - 8) // 2
    owns, others = refs[:plane], refs[plane : 2 * plane]
    gate_w, up_w, expert_gate, expert_up, out, slot_weight, tokens, notes = refs[2 * plane :]
    count = tokens.shape[0]
    half = tokens.shape[1] // 2
    slots = slot_weight.shape[0]
    group = count // plane
    own_part = pl.ds(pl.multiple_of(ids[0] * half, half), half)
    other_part = pl.ds(pl.multiple_of((1 - ids[0]) * half, half), half)
    for j in range(plane):
        rows = pl.ds(j * group, group)
        tokens[rows, own_part] = owns[j][:, :half]
        tokens[rows, other_part] = others[j][:, :half]
        notes[rows, :] = owns[j][:, half:].astype(F32)
    all_rows = tokens[...]
    hidden = silu(dot(all_rows, gate_w[...])) * dot(all_rows, up_w[...])
    out[0:count, 0 : gate_w.shape[1]] = hidden.astype(BF16)
    squares = jnp.sum(hidden * hidden, axis=1, keepdims=True)
    extra = out.shape[0] - count - slots
    tile_row = lax.broadcasted_iota(jnp.int32, (extra, LANES), 0)
    tile = jnp.zeros((extra, LANES), F32)
    for j in range(plane):
        high, low = high_low(to_row(squares[j * group : (j + 1) * group]))
        tile = jnp.where(tile_row == 2 * j, high, jnp.where(tile_row == 2 * j + 1, low, tile))
    out[count + slots :, :] = jnp.zeros((extra, out.shape[1]), BF16)
    out[count + slots :, 0:LANES] = tile.astype(BF16)

    turned = jnp.transpose(notes[...])
    token = axis_iota((1, count), 1)
    token_key = block_of(token, seq) * BLOCK_KEY
    slot = axis_iota((slots, 1), 0)
    slot_block = block_of(slot, capacity)
    slot_key = slot_block * BLOCK_KEY + (slot - slot_block * capacity) + ids[1].astype(F32)
    pick = jnp.zeros((slots, count), F32)
    weight = jnp.zeros((slots, count), F32)
    for k in range(top_k):
        hit = (turned[k : k + 1] + token_key == slot_key).astype(F32)
        value = turned[top_k + k : top_k + k + 1] + turned[2 * top_k + k : 2 * top_k + k + 1]
        pick = pick + hit
        weight = weight + hit * value
    slot_weight[...] = jnp.broadcast_to(
        jnp.sum(weight, axis=1, keepdims=True), slot_weight.shape
    )
    pick = pick.astype(BF16)
    picked = dot(pick, all_rows).astype(BF16)
    active = silu(dot(picked, expert_gate[...])) * dot(picked, expert_up[...])
    out[count : count + slots, 0 : expert_gate.shape[1]] = active.astype(BF16)


def base_kernel(own, down_own, expert_own, dense, routed):
    count, slots = dense.shape[0], routed.shape[0]
    dense[...] = dot(own[0:count, 0 : down_own.shape[0]], down_own[...])
    routed[...] = dot(own[count : count + slots, 0 : expert_own.shape[0]], expert_own[...])


def down_kernel(own, other, dense_base, routed_base, down_got, slot_weight, *outs, hidden):
    plane = len(outs)
    half = outs[0].shape[1]
    count = dense_base.shape[0]
    slots = slot_weight.shape[0]
    routed_hidden = down_got.shape[0] - hidden
    dense = dense_base[...] + dot(other[0:count, 0:hidden], down_got[0:hidden, :])
    routed = routed_base[...] + dot(
        other[count : count + slots, 0:routed_hidden], down_got[hidden:, :]
    )
    routed = routed * slot_weight[:, 0:1]
    squares = own[count + slots :, 0:LANES].astype(F32) + other[count + slots :, 0:LANES].astype(F32)
    group, part = count // plane, slots // plane
    tile_row = lax.broadcasted_iota(jnp.int32, (8, LANES), 0)
    for j in range(plane):
        outs[j][0:group, :] = dense[j * group : (j + 1) * group].astype(BF16)
        outs[j][group : group + part, :] = routed[j * part : (j + 1) * part].astype(BF16)
        high, low = high_low(squares[2 * j : 2 * j + 1] + squares[2 * j + 1 : 2 * j + 2])
        outs[j][group + part :, :] = jnp.zeros((8, half), BF16)
        outs[j][group + part :, 0:LANES] = jnp.where(
            tile_row == 0, high, jnp.where(tile_row == 1, low, 0.0)
        ).astype(BF16)


def plane_kernel(*refs, planes, seq, capacity):
    plane = len(refs) - planes - 1
    parts, combine, outs = refs[:plane], refs[plane], refs[plane + 1 :]
    group, part = planes * seq, planes * capacity
    dense = parts[0][0:group, :].astype(F32)
    routed = dot(combine[0], parts[0][group : group + part, :])
    notes = parts[0][group + part :, 0:LANES].astype(F32)
    for j in range(1, plane):
        dense = dense + parts[j][0:group, :].astype(F32)
        routed = routed + dot(combine[j], parts[j][group : group + part, :])
        notes = notes + parts[j][group + part :, 0:LANES].astype(F32)
    high, low = high_low(notes[0:1] + notes[1:2])
    pair_rows = combine.shape[1] // planes
    tile_row = lax.broadcasted_iota(jnp.int32, (pair_rows, LANES), 0)
    for k in range(planes):
        outs[k][0:seq, :] = dense[k * seq : (k + 1) * seq].astype(BF16)
        tail = routed[k * pair_rows : (k + 1) * pair_rows]
        first = jnp.where(
            tile_row == seq // 2,
            high,
            jnp.where(tile_row == seq // 2 + 1, low, tail[:, 0:LANES]),
        )
        outs[k][seq:, 0:LANES] = first.astype(BF16)
        outs[k][seq:, LANES:] = tail[:, LANES:].astype(BF16)


def final_kernel(*refs, ff_total, route_base, top_k):
    planes = len(refs) - 5
    ids, parts = refs[0], refs[1 : 1 + planes]
    resid, branch, notes, out = refs[1 + planes :]
    seq = resid.shape[0]
    half_seq = seq // 2
    pair_rows = parts[0].shape[0] - seq
    group = block_of(notes[:, 0:1].astype(F32), route_base)
    token_pair = block_of(axis_iota((seq, 1), 0), 2)
    lane = axis_iota((1, pair_rows), 1)
    dense = jnp.zeros(out.shape, F32)
    routed = jnp.zeros(out.shape, F32)
    squares = jnp.zeros((seq, LANES), F32)
    for k in range(planes):
        dense = dense + parts[k][0:seq, :].astype(F32)
        tail = parts[k][seq:, :]
        place = jnp.where(
            (token_pair == lane) & (group == ids[k].astype(F32)), 1.0, 0.0
        ).astype(BF16)
        routed = routed + dot(place, tail)
        values = tail[:, 0:LANES].astype(F32)
        row = values[half_seq : half_seq + 1] + values[half_seq + 1 : half_seq + 2]
        turned = jnp.transpose(jnp.broadcast_to(row, (LANES, LANES)))
        squares = squares + turned[k * seq : (k + 1) * seq]
    scale = branch[:, 0:1] * lax.rsqrt(squares[:, 0:1] * (1.0 / ff_total) + norm_eps)
    out[...] = (resid[...].astype(F32) + routed + scale * dense).astype(BF16)


def attend_kernel(
    ids, lens_in, tokens_in, norm_in, query_in, key_in, bias_in,
    query_w, key_w, value_w, forget_w, cache_key, cache_value, cache_gate, out_w,
    partial, fresh_key, fresh_value, fresh_gate,
    q_w, k_w, v_w, f_w, keys, values, gates, o_w, q_rows, k_rows, v_rows, f_cols, g_cols, mixed,
    tokens, norm_gain, query_gain, key_gain, forget_bias, lens, sems,
    *, heads, chunks,
):
    seq = tokens.shape[0]
    head = cache_key.shape[1]
    span = cache_key.shape[2]
    step = seq // chunks
    plain = [
        (tokens_in, tokens), (norm_in, norm_gain), (query_in, query_gain), (key_in, key_gain),
        (bias_in, forget_bias), (lens_in, lens), (key_w, k_w), (value_w, v_w), (forget_w, f_w), (query_w, q_w),
    ]
    small = [pltpu.make_async_copy(a, b, sems.at[i]) for i, (a, b) in enumerate(plain)]
    base = len(small)
    parts = []
    for c in range(chunks):
        rows = pl.ds(c * step, step)
        for a, b in ((cache_key, keys), (cache_gate, gates), (cache_value, values)):
            parts.append(pltpu.make_async_copy(a.at[rows], b.at[rows], sems.at[base + len(parts)]))
    last = pltpu.make_async_copy(out_w, o_w, sems.at[base + len(parts)])
    for copy in small + parts + [last]:
        copy.start()
    for copy in small[:6]:
        copy.wait()
    small = small[6:]
    first = ids[0] == 0
    resid = tokens[...].astype(F32)
    mean_square = jnp.mean(resid * resid, axis=-1, keepdims=True)
    normed = (resid * lax.rsqrt(mean_square + norm_eps) * norm_gain[...].astype(F32)[None]).astype(BF16)
    small[0].wait()
    key = dot(normed, k_w[...])
    key = jnp.where(first, key[:, :head], key[:, head:])
    key = rms_scale(key, key_gain[...].astype(F32)[None]).astype(BF16)
    fresh_key[...] = key
    k_rows[...] = key.astype(F32)
    small[1].wait()
    value = dot(normed, v_w[...])
    value = jnp.where(first, value[:, :head], value[:, head:]).astype(BF16)
    fresh_value[...] = value
    v_rows[...] = value.astype(F32)
    small[2].wait()
    forget = lax.dot_general(
        normed, f_w[...], (((1,), (1,)), ((), ())), preferred_element_type=F32
    )
    forget = forget + forget_bias[...][None]
    forget = jnp.minimum(forget, 0.0) - jnp.log1p(jnp.exp(-jnp.abs(forget)))
    forget = jnp.where(first, forget[:, :heads], forget[:, heads:])
    wide = jnp.concatenate([forget, jnp.zeros((seq, LANES - heads), F32)], axis=1)
    wide = jnp.concatenate([wide, jnp.zeros((LANES - seq, LANES), F32)], axis=0)
    f_cols[...] = jnp.transpose(wide)[0:heads]
    small[3].wait()
    queries = dot(normed, q_w[...])
    scale = head ** (-0.5)
    for h in range(heads):
        part = queries[:, h * head : (h + 1) * head]
        part = rms_scale(part, query_gain[...].astype(F32)[None]).astype(BF16)
        q_rows[:, h, :] = part.astype(F32) * scale
    g_cols[...] = jnp.zeros(g_cols.shape, F32)
    lane = lax.broadcasted_iota(jnp.int32, (heads, span), 1)
    lane_small = lax.broadcasted_iota(jnp.int32, (heads, LANES), 1)

    def several(span_of):
        lengths = [lens[s] for s in span_of]
        place = [length - 1 for length in lengths]
        block = [pl.multiple_of((at // LANES) * LANES, LANES) for at in place]
        near = [gates[s, :, pl.ds(at, LANES)] for s, at in zip(span_of, block)]
        previous = [
            jnp.sum(jnp.where(lane_small == at - start, value, 0.0), axis=1, keepdims=True)
            for at, start, value in zip(place, block, near)
        ]
        current = [f_cols[:, s : s + 1] + value for s, value in zip(span_of, previous)]
        for s, value in zip(span_of, current):
            g_cols[:, s : s + 1] = value
        query = [q_rows[s] for s in span_of]
        scores = [dot(value.astype(BF16), keys[s]) for s, value in zip(span_of, query)]
        own = [
            jnp.sum(value * k_rows[s : s + 1], axis=1, keepdims=True)
            for s, value in zip(span_of, query)
        ]
        logits = [
            jnp.where(lane < length, score + (now - gates[s]), -1e30)
            for s, length, score, now in zip(span_of, lengths, scores, current)
        ]
        top = [
            jnp.maximum(jnp.max(value, axis=1, keepdims=True), mine)
            for value, mine in zip(logits, own)
        ]
        weight = [jnp.exp(value - peak) for value, peak in zip(logits, top)]
        own_weight = [jnp.exp(mine - peak) for mine, peak in zip(own, top)]
        inverse = [
            1.0 / (jnp.sum(value, axis=1, keepdims=True) + mine)
            for value, mine in zip(weight, own_weight)
        ]
        probs = [(value * factor).astype(BF16) for value, factor in zip(weight, inverse)]
        out = [
            lax.dot_general(
                value, values[s], (((1,), (1,)), ((), ())), preferred_element_type=F32
            )
            for s, value in zip(span_of, probs)
        ]
        for s, value, mine, factor in zip(span_of, out, own_weight, inverse):
            own_prob = (mine * factor).astype(BF16).astype(F32)
            mixed[s] = value + own_prob * v_rows[s : s + 1]

    for c in range(chunks):
        for copy in parts[3 * c : 3 * c + 3]:
            copy.wait()
        for start in range(c * step, (c + 1) * step, 12):
            several(range(start, min(start + 12, (c + 1) * step)))
    turned = jnp.concatenate([g_cols[...], jnp.zeros((LANES - heads, LANES), F32)], axis=0)
    fresh_gate[...] = jnp.transpose(turned)[0:seq, 0:heads]
    last.wait()
    total = jnp.zeros(partial.shape, F32)
    for h in range(heads):
        total = total + dot(mixed[:, h, :].astype(BF16), o_w[h * head : (h + 1) * head, :])
    partial[...] = total.astype(BF16)


def attend(
    ids, tokens, norm_gain, query_w, key_w, value_w, forget_w, forget_bias,
    query_gain, key_gain, cache_key, cache_value, cache_gate, cache_len, out_w,
):
    seq, width = tokens.shape
    heads = cache_gate.shape[1]
    head, span = cache_key.shape[2:]
    chunks = 2 if seq % 2 == 0 else 1
    scratch = [
        pltpu.VMEM(query_w.shape, BF16), pltpu.VMEM(key_w.shape, BF16),
        pltpu.VMEM(value_w.shape, BF16), pltpu.VMEM(forget_w.shape[::-1], BF16),
        pltpu.VMEM((seq, head, span), BF16), pltpu.VMEM((seq, head, span), BF16),
        pltpu.VMEM((seq, heads, span), F32), pltpu.VMEM(out_w.shape, BF16),
        pltpu.VMEM((seq, heads, head), F32), pltpu.VMEM((seq, head), F32),
        pltpu.VMEM((seq, head), F32), pltpu.VMEM((heads, LANES), F32),
        pltpu.VMEM((heads, LANES), F32), pltpu.VMEM((seq, heads, head), F32),
        pltpu.VMEM(tokens.shape, BF16), pltpu.VMEM(norm_gain.shape, BF16),
        pltpu.VMEM(query_gain.shape, BF16), pltpu.VMEM(key_gain.shape, BF16),
        pltpu.VMEM(forget_bias.shape, F32), pltpu.SMEM(cache_len.shape, jnp.int32),
        pltpu.SemaphoreType.DMA((11 + 3 * chunks,)),
    ]
    partial, fresh_key, fresh_value, current = call(
        functools.partial(attend_kernel, heads=heads, chunks=chunks),
        [((seq, width), BF16), ((seq, head), BF16), ((seq, head), BF16), ((seq, heads), F32)],
        [
            ids, cache_len, tokens, norm_gain, query_gain, key_gain, forget_bias, query_w, key_w, value_w, forget_w.T,
            cache_key[:, 0], cache_value[:, 0], cache_gate, out_w,
        ],
        hbm=range(1, 15),
        scratch=scratch,
        limit=32,
    )
    return partial, fresh_key[:, None], fresh_value[:, None], current


def body(
    tokens, norm_gain, query_w, key_w, value_w, forget_w, forget_bias, query_gain, key_gain,
    cache_key, cache_value, cache_gate, cache_len, out_w, post_gain, branch_gate,
    dense_gate_w, dense_up_w, dense_down_w, expert_choice, route_weight,
    expert_gate_w, expert_up_w, expert_down_w,
):
    seq, width = tokens.shape
    tp_count = lax.axis_size("tp")
    ep_count = lax.axis_size("ep")
    tp_rank = lax.axis_index("tp")
    ep_rank = lax.axis_index("ep")
    half = width // tp_count
    planes = GROUPS
    plane = ep_count // planes
    capacity = 2 * ((seq + 2 * plane - 1) // (2 * plane))
    top_k = expert_choice.shape[1]
    ff_local = dense_gate_w.shape[1]
    expert_local = expert_gate_w.shape[2]
    widest = max(ff_local, expert_local)
    ff_total = ff_local * ep_count * tp_count
    pair_rows = 8 * ((seq // 2 + 2 + 7) // 8)
    z_rank = ep_rank // plane
    p_rank = ep_rank % plane

    def swap(values):
        return lax.ppermute(values, "tp", [(i, 1 - i) for i in range(tp_count)])

    def exchange(values, mask):
        return lax.ppermute(values, "ep", [(i, i ^ mask) for i in range(ep_count)])

    slot_ids = route_slots(expert_choice, ep_count, capacity)
    weight_high, weight_low = split_two(route_weight)
    notes = jnp.concatenate([slot_ids.astype(BF16), weight_high, weight_low], axis=1)
    notes = jnp.pad(notes, ((0, 0), (0, LANES - notes.shape[1])))
    peers = jnp.bitwise_xor(jnp.arange(plane, dtype=jnp.int32), p_rank) + z_rank * plane
    ids = jnp.concatenate([jnp.stack([tp_rank, ep_rank * capacity]), peers * capacity])
    ids = ids.astype(jnp.int32)
    z_peers = jnp.bitwise_xor(jnp.arange(planes, dtype=jnp.int32), z_rank)

    partial, fresh_key, fresh_value, current = attend(
        ids, tokens, norm_gain, query_w, key_w, value_w, forget_w, forget_bias,
        query_gain, key_gain, cache_key, cache_value, cache_gate, cache_len, out_w,
    )
    payload, resid, branch = call(
        post_kernel,
        [((seq, half + LANES), BF16), ((seq, half), BF16), ((seq, LANES), F32)],
        [ids, tokens, partial, swap(partial), post_gain, branch_gate, notes],
    )
    near = [None] * planes
    for k in reversed(range(1, planes)):
        near[k] = exchange(payload, k * plane)
    wide = [dense_gate_w, dense_up_w, expert_gate_w[0], expert_up_w[0]]
    down_sent, gate_w, up_w, expert_gate, expert_up = call(
        fetch_kernel,
        [((ff_local + expert_local, half), BF16)] + [(value.shape, BF16) for value in wide],
        [ids, payload, *wide, dense_down_w, expert_down_w[0]],
        hbm=range(2, 8),
        scratch=[pltpu.SemaphoreType.DMA((6,))],
    )
    column = jnp.concatenate([payload] + near[1:], axis=0)
    owns = [column] + [None] * (plane - 1)
    for j in reversed(range(1, plane)):
        owns[j] = exchange(column, j)
    down_own, expert_own = call(
        load_kernel,
        [((ff_local, half), BF16), ((expert_local, half), BF16)],
        [ids, column, dense_down_w, expert_down_w[0]],
        hbm=range(2, 4),
        scratch=[pltpu.SemaphoreType.DMA((2,))],
    )
    (combine,) = call(
        functools.partial(table_kernel, seq=seq, capacity=capacity, top_k=top_k),
        [((plane, planes * pair_rows, planes * capacity), BF16)],
        [ids, column],
    )
    down_got = swap(down_sent)
    others = []
    for j in range(plane):
        others.append(swap(owns[j]))
    arrived = [None] * plane
    order = list(reversed(range(1, plane)))
    early, late = order[: plane // 2 - 1], order[plane // 2 - 1 :]
    for members in ([0] + early, late):
        size = len(members)
        rows, routes = size * planes * seq, size * planes * capacity
        extra = 8 * ((2 * size + 7) // 8)
        hidden, slot_weight = call(
            functools.partial(hidden_kernel, seq=seq, capacity=capacity, top_k=top_k),
            [((rows + routes + extra, widest), BF16), ((routes, LANES), F32)],
            [
                ids, *[owns[j] for j in members], *[others[j] for j in members],
                gate_w, up_w, expert_gate, expert_up,
            ],
            scratch=[
                pltpu.VMEM((rows, width), BF16), pltpu.VMEM((rows, LANES), F32),
            ],
        )
        hidden_other = swap(hidden)
        dense_base, routed_base = call(
            base_kernel,
            [((rows, half), F32), ((routes, half), F32)],
            [hidden, down_own, expert_own],
        )
        sums = call(
            functools.partial(down_kernel, hidden=ff_local),
            [((planes * (seq + capacity) + 8, half), BF16)] * size,
            [hidden, hidden_other, dense_base, routed_base, down_got, slot_weight],
        )
        for j, value in zip(members, sums):
            arrived[j] = exchange(value, j) if j else value
    lasts = call(
        functools.partial(plane_kernel, planes=planes, seq=seq, capacity=capacity),
        [((seq + pair_rows, half), BF16)] * planes,
        [*arrived, combine],
    )
    final = [lasts[0]] + [None] * (planes - 1)
    for k in reversed(range(1, planes)):
        final[k] = exchange(lasts[k], k * plane)
    (mixed_out,) = call(
        functools.partial(
            final_kernel, ff_total=ff_total, route_base=capacity * plane, top_k=top_k
        ),
        [((seq, half), BF16)],
        [z_peers, *final, resid, branch, notes],
        kept=True,
    )
    return (mixed_out, fresh_key, fresh_value, current)


def solution(mesh):
    placed = (
        P("ep", None), P(), P(None, "tp"), P(), P(), P(), P(), P(), P(),
        P("ep", "tp", None, None), P("ep", "tp", None, None), P("ep", "tp", None), P("ep"),
        P("tp", None), P(), P(),
        P(None, ("ep", "tp")), P(None, ("ep", "tp")), P(("ep", "tp"), None),
        P("ep", None), P("ep", None),
        P("ep", None, "tp"), P("ep", None, "tp"), P("ep", "tp", None),
    )
    return jax.shard_map(
        body,
        mesh=mesh,
        in_specs=placed,
        out_specs=(P("ep", "tp"), P("ep", "tp", None), P("ep", "tp", None), P("ep", "tp")),
        check_vma=False,
    )
```
